512 devices in a mesh: ep: 32 (over z, core), tp: 16 (over y, x).
Axes of the slice: x: 4, y: 4, z: 16, core: 2. Of those that a mesh axis runs over, the one named last changes fastest.
Arguments:
- query_input: bfloat16 [16384, 2048], P('ep', 'tp'), may hold values from -6 to 6
- key_input: bfloat16 [16384, 1024], P('ep', 'tp'), may hold values from -6 to 6
- value_input: bfloat16 [16384, 1024], P('ep', 'tp'), may hold values from -64 to 64
- query_gain: float32 [64], replicated, may hold values from 0.5 to 6
- key_gain: float32 [64], replicated, may hold values from 0.5 to 6
- mixer_out: bfloat16 [2048, 4096], P(None, 'tp'), may hold values from -0.125 to 0.125
- moe_input: bfloat16 [8192, 4096], P('ep'), may hold values from -6 to 6
- moe_gain: float32 [4096], replicated, may hold values from 0.1 to 1.9
- routes: int32 [8192, 2], P('ep'), may hold values from 0 to 31, all different within a row; in each aligned block of 256 rows (0 to 255, 256 to 511, ...) at most 24 rows name the same one
- route_weight: float32 [8192, 2], P('ep'), may hold values from 0.1 to 1
- expert_gate: bfloat16 [32, 4096, 1024], P('ep', None, 'tp'), may hold values from -0.09375 to 0.09375
- expert_up: bfloat16 [32, 4096, 1024], P('ep', None, 'tp'), may hold values from -0.09375 to 0.09375
- expert_down: bfloat16 [32, 1024, 4096], P('ep', None, 'tp'), may hold values from -0.1875 to 0.1875
Outputs:
- attn_mixed: bfloat16 [16384, 4096], P('ep', 'tp')
- moe_out: bfloat16 [8192, 4096], P('ep', 'tp')
The draws below stay inside these ranges and needn't reach their ends.
Inputs may be any that keep to these rules, and one draw needn't show every extreme that they name: `routes`: each row names 2 different experts. In the rows of one index of ep (aligned blocks of 256 rows) no expert is named by more than 24 rows, and in every draw some block has an expert named by exactly 24 rows.
All inputs are finite; a program needn't handle non-finite values.
Results may differ from the reference program's by a relative error of at most 0.0095.
The reference program's roundings to bfloat16 on the way count: a program that leaves them out, or rounds other values in their place, can miss the bound.
Values may be sent and summed in bfloat16 or wider, within the bound.
A program may use at most 64 MiB of HBM per device.

```python
import math
import jax
import jax.numpy as jnp
import numpy as np
from jax import lax

D = 4096
HEADS = 32
KV_HEADS = 16
HEAD_DIM = 64
FF = 1024
GRID_W = 64
TOP_K = 2
MOE_TOK = 256
SEQ_LEN = 16384
MOE_TOKENS = 8192
EXPERTS = 32
CAP = 24
N_EP = 32


def draw_query_input(key, part):
    column_count = HEADS * HEAD_DIM
    samples = jnp.clip(jax.random.normal(jax.random.fold_in(key, 101), (SEQ_LEN, column_count), jnp.float32), -6.0, 6.0)
    return samples.astype(jnp.bfloat16)


def draw_key_input(key, part):
    column_count = KV_HEADS * HEAD_DIM
    samples = jnp.clip(jax.random.normal(jax.random.fold_in(key, 202), (SEQ_LEN, column_count), jnp.float32), -6.0, 6.0)
    return samples.astype(jnp.bfloat16)


def draw_query_gain(key, part):
    spread = jax.random.uniform(jax.random.fold_in(key, 303), (HEAD_DIM,), jnp.float32, jnp.log(0.5), jnp.log(2.0))
    gains = jnp.exp(spread)
    return gains.astype(jnp.float32)


def draw_key_gain(key, part):
    spread = jax.random.uniform(jax.random.fold_in(key, 404), (HEAD_DIM,), jnp.float32, jnp.log(0.5), jnp.log(2.0))
    gains = jnp.exp(spread)
    return gains.astype(jnp.float32)


def block_levels(key, shape, pieces, least, high):
    def one(axis_at, blocks):
        heights = jax.random.uniform(jax.random.fold_in(jax.random.fold_in(key, 6), axis_at), (blocks,), jnp.float32, least / len(pieces), high / len(pieces))
        return jnp.repeat(jnp.exp(heights), shape[axis_at] // blocks).reshape((-1,) + (1,) * (len(shape) - axis_at - 1))

    factor_of = one(*pieces[0])
    for cut in pieces[1:]:
        factor_of = factor_of * one(*cut)
    return factor_of


def routed_block(stream_key, own, number, rows, amount, top, bound, skew):
    order = jax.random.permutation(stream_key, amount)
    packed, common = portions_of(amount, rows * top, bound, skew, True), portions_of(amount, rows * top, bound, skew, False)
    places = jnp.arange(amount)

    def named(tallies, rotation):
        used = int((tallies > 0).sum())
        fixed = max(1, used // 4)
        moved = fixed + (places - fixed + rotation * (used - fixed)) % max(1, amount - fixed)
        return jnp.zeros((amount,), jnp.int32).at[order[jnp.where(places < fixed, places, moved)]].set(jnp.asarray(tallies, jnp.int32))

    tallies = jnp.where(number % 4 == 0, named(packed, number // 4), named(common, number - number // 4 - 1))
    mixed = jax.random.permutation(jax.random.fold_in(own, 3), amount)
    source_of, sink = mixed[0:amount // 2 * 2:2], mixed[1:amount // 2 * 2:2]
    slack = jnp.minimum(tallies[source_of] - 1, bound - tallies[sink]) // 2
    slack = jnp.where((source_of == order[0]) | (sink == order[0]) | (tallies[sink] == 0), 0, jnp.maximum(slack, 0))
    moved = jax.random.randint(jax.random.fold_in(own, 4), (amount // 2,), 0, 1 << 20) % (slack + 1)
    tallies = tallies.at[source_of].add(-moved).at[sink].add(moved)
    labels = jnp.searchsorted(jnp.cumsum(tallies), jnp.arange(rows * top), side="right").astype(jnp.int32)
    listing = labels.reshape(top, rows).T
    listing = listing[jax.random.permutation(jax.random.fold_in(own, 1), rows)]
    rotation = jax.random.randint(jax.random.fold_in(own, 2), (rows, 1), 0, top)
    return jnp.take_along_axis(listing, (jnp.arange(top)[None, :] + rotation) % top, axis=1)


def portions_of(amount, total, reach, skew, full):
    weights = [(1 << 20) // math.isqrt(rank ** skew) + 1 for rank in range(1, amount + 1)]
    largest = reach if full else min(reach, max(-(-total // amount), total * weights[0] // sum(weights)))
    least = 1 if total - largest >= amount - 1 else 0
    counts, rest = [largest] + [least] * (amount - 1), total - largest - least * (amount - 1)
    while rest > 0:
        movable = [i for i in range(1, amount) if counts[i] < largest] or [i for i in range(1, amount) if counts[i] < reach]
        pool, left = sum([weights[i] for i in movable]), rest
        for i in movable:
            addition = min(reach - counts[i], max(1, left * weights[i] // pool), rest)
            counts[i] = counts[i] + addition
            rest = rest - addition
    return np.array(counts)


def scatter_about(stream_key, dims, scale, bound, cuts=(), held_as=jnp.bfloat16):
    result = jax.random.normal(stream_key, dims, jnp.float32) * scale
    if len(cuts) > 0:
        result = block_levels(stream_key, dims, cuts, -0.22, 0.18) * result
    return jnp.clip(result, min=-bound, max=bound).astype(held_as)


def setup_inputs(seed: int = 0) -> dict:
    streams_of = jax.random.split(jax.random.key(seed), 14)
    query_input = draw_query_input(jax.random.fold_in(streams_of[13], 71), 0)
    key_input = draw_key_input(jax.random.fold_in(streams_of[13], 71), 0)
    value_input = jnp.clip(jax.random.uniform(streams_of[2], (SEQ_LEN, KV_HEADS * HEAD_DIM), jnp.float32, -64.0, 64.0) * block_levels(streams_of[2], (SEQ_LEN, KV_HEADS * HEAD_DIM), ((0, 32), (1, 16)), -0.4, 0.0), -64.0, 64.0).astype(jnp.bfloat16)
    query_gain = draw_query_gain(jax.random.fold_in(streams_of[13], 71), 0)
    key_gain = draw_key_gain(jax.random.fold_in(streams_of[13], 71), 0)
    mixer_out = scatter_about(streams_of[5], (HEADS * HEAD_DIM, D), (HEADS * HEAD_DIM) ** -0.5, 0.125, ((1, 16),))
    moe_input = scatter_about(streams_of[6], (MOE_TOKENS, D), 1.0, 6.0, ((0, 32),))
    moe_gain = jnp.clip(1.0 + 0.18 * jax.random.normal(streams_of[7], (D,), jnp.float32), 0.1, 1.9)
    routes_keys = jax.random.split(jax.random.fold_in(streams_of[8], 1), MOE_TOKENS // MOE_TOK)
    routes_turns = jax.random.permutation(jax.random.fold_in(streams_of[8], 3), MOE_TOKENS // MOE_TOK)
    routes = jax.vmap(lambda own, number: routed_block(jax.random.fold_in(streams_of[8], 2), own, number, MOE_TOK, EXPERTS, TOP_K, CAP, 1))(routes_keys, routes_turns).reshape((MOE_TOKENS, TOP_K))
    route_weight = jnp.clip(jnp.exp(math.log(1.0) - 2.3025851 * jax.random.uniform(streams_of[9], (MOE_TOKENS, TOP_K), jnp.float32) ** block_levels(streams_of[9], (MOE_TOKENS, TOP_K), ((0, 32),), -0.2, 0.2)), 0.1, 1.0)
    expert_gate = scatter_about(streams_of[10], (EXPERTS, D, FF), D ** -0.5, 0.09375, ((0, 32), (2, 16)))
    expert_up = scatter_about(streams_of[11], (EXPERTS, D, FF), D ** -0.5, 0.09375, ((0, 32), (2, 16)))
    expert_down = scatter_about(streams_of[12], (EXPERTS, FF, D), FF ** -0.5, 0.1875, ((0, 32), (2, 16)))
    return {"query_input": query_input, "key_input": key_input, "value_input": value_input, "query_gain": query_gain, "key_gain": key_gain, "mixer_out": mixer_out, "moe_input": moe_input, "moe_gain": moe_gain, "routes": routes, "route_weight": route_weight, "expert_gate": expert_gate, "expert_up": expert_up, "expert_down": expert_down}


epsilon = 1e-06
base_theta = 10000.0

def rope_tables(positions, head_width):
    quarter = head_width // 4
    inverse = base_theta ** (-jnp.arange(quarter, dtype=jnp.float32) / quarter)
    grid_row = (positions // GRID_W).astype(jnp.float32)
    grid_col = (positions % GRID_W).astype(jnp.float32)
    angles = jnp.concatenate([grid_row[:, None] * inverse[None, :], grid_col[:, None] * inverse[None, :]], axis=1)
    return (jnp.cos(angles), jnp.sin(angles))

def head_norm(heads_in, gain):
    return heads_in * lax.rsqrt(lax.optimization_barrier(jnp.mean(heads_in * heads_in, axis=-1, keepdims=True)) + epsilon) * gain

def rotate(heads_in, cosine, sine_table):
    half_width = heads_in.shape[-1] // 2
    first_half = heads_in[..., :half_width]
    second_half = heads_in[..., half_width:]
    cos_rows = cosine[:, None, :]
    sin_rows = sine_table[:, None, :]
    return jnp.concatenate([first_half * cos_rows - second_half * sin_rows, first_half * sin_rows + second_half * cos_rows], axis=-1)

def slot_places(route_block, expert_count, capacity):
    flat_routes = route_block.reshape(-1)
    one_hot = (flat_routes[:, None] == jnp.arange(expert_count, dtype=jnp.int32)[None, :]).astype(jnp.int32)
    earlier = jnp.cumsum(one_hot, axis=0) - one_hot
    return (flat_routes * capacity + lax.optimization_barrier(jnp.sum(earlier * one_hot, axis=1))).astype(jnp.int32)

def fill_sources(places, token_count, top_count, slot_total):
    source_rows = jnp.full((slot_total,), token_count, jnp.int32)
    pair_rows = (jnp.arange(token_count * top_count, dtype=jnp.int32) // top_count).astype(jnp.int32)
    return source_rows.at[places].set(pair_rows)

def attend(query_rot, key_rot, value_input):
    seq_len = query_rot.shape[0]
    group_size = HEADS // KV_HEADS
    block_len = math.gcd(seq_len, 128)
    key_all = key_rot.astype(jnp.float32)
    value_all = value_input.astype(jnp.float32).reshape(seq_len, KV_HEADS, HEAD_DIM)
    blocks = query_rot.astype(jnp.float32).reshape(seq_len // block_len, block_len, KV_HEADS, group_size, HEAD_DIM)
    score_scale = HEAD_DIM ** (-0.5)

    def one_block(query_block):
        scores = jnp.einsum('qkgd,skd->kgqs', query_block, key_all) * score_scale
        largest = lax.optimization_barrier(jnp.max(scores, axis=-1, keepdims=True))
        weights = jnp.exp(scores - largest)
        denominator = lax.optimization_barrier(jnp.sum(weights, axis=-1))
        rounded = lax.optimization_barrier(weights.astype(jnp.bfloat16)).astype(jnp.float32)
        numerator = jnp.einsum('kgqs,skd->qkgd', rounded, value_all)
        return numerator / jnp.transpose(denominator, (2, 0, 1))[..., None]
    attended = lax.map(one_block, blocks)
    return attended.reshape(seq_len, HEADS * HEAD_DIM).astype(jnp.bfloat16)

def experts_layer(moe_input, moe_gain, routes, route_weight, expert_gate, expert_up, expert_down):
    features = moe_input.astype(jnp.float32)
    normed = (features * lax.rsqrt(lax.optimization_barrier(jnp.mean(features * features, axis=-1, keepdims=True)) + epsilon) * moe_gain).astype(jnp.bfloat16)
    blocks = normed.reshape(N_EP, MOE_TOK, D)
    places = jax.vmap(lambda route_block: slot_places(route_block, EXPERTS, CAP))(routes.reshape(N_EP, MOE_TOK, TOP_K))
    sources = jax.vmap(lambda place_row: fill_sources(place_row, MOE_TOK, TOP_K, EXPERTS * CAP))(places)
    padded = jnp.concatenate([blocks, jnp.zeros((N_EP, 1, D), jnp.bfloat16)], axis=1)
    gathered = jax.vmap(lambda padded_block, source_row: padded_block[source_row])(padded, sources)
    per_expert = gathered.reshape(N_EP, EXPERTS, CAP, D).transpose(1, 0, 2, 3).reshape(EXPERTS, N_EP * CAP, D)

    def one_expert(operands):
        expert_rows, gate_matrix, up_matrix, down_matrix = operands
        gate_hidden = jnp.dot(expert_rows, gate_matrix, preferred_element_type=jnp.float32)
        up_hidden = jnp.dot(expert_rows, up_matrix, preferred_element_type=jnp.float32)
        hidden = (jax.nn.silu(gate_hidden) * up_hidden).astype(jnp.bfloat16)
        return jnp.dot(hidden, down_matrix, preferred_element_type=jnp.float32).astype(jnp.bfloat16)
    outputs = lax.map(one_expert, (per_expert, expert_gate, expert_up, expert_down))
    returned = outputs.reshape(EXPERTS, N_EP, CAP, D).transpose(1, 0, 2, 3).reshape(N_EP, EXPERTS * CAP, D)
    picked = jax.vmap(lambda returned_block, place_row: returned_block[place_row])(returned, places)
    picked = picked.reshape(N_EP * MOE_TOK, TOP_K, D).astype(jnp.float32)
    shares = route_weight / lax.optimization_barrier(jnp.sum(route_weight, axis=-1, keepdims=True))
    return lax.optimization_barrier(jnp.sum(picked * shares[:, :, None], axis=1)).astype(jnp.bfloat16)

def reference(query_input, key_input, value_input, query_gain, key_gain, mixer_out, moe_input, moe_gain, routes, route_weight, expert_gate, expert_up, expert_down):
    seq_len = query_input.shape[0]
    positions = jnp.arange(seq_len, dtype=jnp.int32)
    cosine, sine_table = rope_tables(positions, HEAD_DIM)
    query_heads = query_input.astype(jnp.float32).reshape(seq_len, HEADS, HEAD_DIM)
    key_heads = key_input.astype(jnp.float32).reshape(seq_len, KV_HEADS, HEAD_DIM)
    query_rot = rotate(head_norm(query_heads, query_gain), cosine, sine_table).astype(jnp.bfloat16)
    key_rot = rotate(head_norm(key_heads, key_gain), cosine, sine_table).astype(jnp.bfloat16)
    attended = attend(query_rot, key_rot, value_input)
    attn_mixed = jnp.dot(attended, mixer_out, preferred_element_type=jnp.float32).astype(jnp.bfloat16)
    moe_out = experts_layer(moe_input, moe_gain, routes, route_weight, expert_gate, expert_up, expert_down)
    return (attn_mixed, moe_out)
```

```python
import functools

import jax
import jax.numpy as jnp
from jax import lax
from jax.experimental import pallas as pl
from jax.experimental.pallas import tpu as pltpu
from jax.sharding import Mesh
from jax.sharding import PartitionSpec as P

GRID_W = 64
TP = ("tp_0", "tp_1")


epsilon = 1e-06
base_theta = 10000.0


def gather_axes(x, axes, dim):
    for axis in reversed(axes):
        x = lax.all_gather(x, axis, axis=dim, tiled=True)
    return x


def copy_for_each(x, axis):
    copies = jnp.broadcast_to(x, (lax.axis_size(axis), *x.shape))
    return lax.all_to_all(copies, axis, split_axis=0, concat_axis=0, tiled=True)


def joined_along(parts, dim):
    parts = jnp.moveaxis(parts, 0, dim)
    shape = parts.shape
    return parts.reshape(*shape[:dim], shape[dim] * shape[dim + 1], *shape[dim + 2 :])


def gathered_copies(x, axis, dim):
    parts = copy_for_each(x, axis)
    return joined_along(parts, dim)


def rope_tables(positions, head_width):
    quarter = head_width // 4
    inverse = base_theta ** (-jnp.arange(quarter, dtype=jnp.float32) / quarter)
    grid_row = (positions // GRID_W).astype(jnp.float32)
    grid_col = (positions % GRID_W).astype(jnp.float32)
    angles = jnp.concatenate(
        [inverse[:, None] * grid_row[None, :], inverse[:, None] * grid_col[None, :]], axis=0
    )
    return (jnp.cos(angles), jnp.sin(angles))


def rotated(x, cosine, sine, gain):
    scale = lax.rsqrt(jnp.mean(x * x, axis=0, keepdims=True) + epsilon)
    x = x * scale * gain
    half = x.shape[0] // 2
    first, second = x[:half], x[half:]
    return jnp.concatenate(
        [first * cosine - second * sine, first * sine + second * cosine], axis=0
    )


def key_value_kernel(width, k_ref, v_ref, cos_ref, sin_ref, gain_ref, out_ref):
    k_t = k_ref[...].astype(jnp.float32).T
    k_t = rotated(k_t, cos_ref[...], sin_ref[...], gain_ref[...])
    v = v_ref[...].astype(jnp.float32)
    out_ref[...] = jnp.concatenate([k_t.T, v], axis=1).astype(jnp.bfloat16)


def flash_kernel(
    width, block, q_ref, kv_ref, cos_ref, sin_ref, gain_ref, out_ref, qt_ref, s_ref, mx_ref, m_ref, o_ref
):
    rows = q_ref.shape[0]
    heads = q_ref.shape[1] // width
    lanes = heads * rows
    blocks = kv_ref.shape[0] // block
    q_t = q_ref[...].astype(jnp.float32).T
    for head in range(heads):
        turned = rotated(
            q_t[head * width : (head + 1) * width], cos_ref[...], sin_ref[...], gain_ref[...]
        )
        turned = turned.astype(jnp.bfloat16).astype(jnp.float32) * (width ** (-0.5))
        qt_ref[:width, head * rows : (head + 1) * rows] = turned.astype(jnp.bfloat16)
    qt_ref[width:, :] = jnp.zeros((width, lanes), jnp.bfloat16)
    m_ref[...] = jnp.full(m_ref.shape, -1e30, jnp.float32)
    o_ref[...] = jnp.zeros(o_ref.shape, jnp.float32)
    log2e = 1.4426950408889634

    def scores(index, slot):
        keys = kv_ref[pl.ds(pl.multiple_of(index * block, block), block), :]
        s = jnp.dot(keys, qt_ref[...], preferred_element_type=jnp.float32)
        s_ref[slot] = s
        mx_ref[slot] = jnp.max(s.reshape(block // 8, 8, lanes), axis=0)

    def absorb(index, slot):
        old = m_ref[...]
        new = jnp.maximum(old, jnp.max(mx_ref[slot], axis=0, keepdims=True) * log2e)
        m_ref[...] = new
        factor = jnp.exp2(old - new)
        p = jnp.exp2(s_ref[slot] * log2e - new[:1]).astype(jnp.bfloat16)
        kv = kv_ref[pl.ds(pl.multiple_of(index * block, block), block), :]
        v_t = kv.T[width:]
        lhs = jnp.concatenate([jnp.ones((16, block), jnp.bfloat16), v_t], axis=0)
        part = jnp.dot(lhs, p, preferred_element_type=jnp.float32)
        o_ref[...] = o_ref[...] * factor[:1] + part

    scores(0, 0)

    @pl.loop(0, blocks - 1)
    def _(index):
        slot = lax.rem(index, 2)
        scores(index + 1, 1 - slot)
        absorb(index, slot)

    absorb(blocks - 1, (blocks - 1) % 2)
    attended = o_ref[16:, :] / o_ref[:1, :]
    for head in range(heads):
        out_ref[:, head * width : (head + 1) * width] = (
            attended[:, head * rows : (head + 1) * rows].T.astype(jnp.bfloat16)
        )


def vmem():
    return pl.BlockSpec(memory_space=pltpu.VMEM)


def key_value_rows(key_input, value_input, cosine, sine, gain):
    rows, width = key_input.shape
    return pl.pallas_call(
        functools.partial(key_value_kernel, width),
        out_shape=jax.ShapeDtypeStruct((rows, 2 * width), jnp.bfloat16),
        in_specs=[vmem()] * 5,
        out_specs=vmem(),
    )(key_input, value_input, cosine, sine, gain)


def flash(query_input, key_values, cosine, sine, gain):
    rows, columns = query_input.shape
    width = gain.shape[0]
    lanes = rows * (columns // width)
    block = 512
    return pl.pallas_call(
        functools.partial(flash_kernel, width, block),
        out_shape=jax.ShapeDtypeStruct((rows, columns), jnp.bfloat16),
        in_specs=[vmem()] * 5,
        out_specs=vmem(),
        scratch_shapes=[
            pltpu.VMEM((2 * width, lanes), jnp.bfloat16),
            pltpu.VMEM((2, block, lanes), jnp.float32),
            pltpu.VMEM((2, 8, lanes), jnp.float32),
            pltpu.VMEM((8, lanes), jnp.float32),
            pltpu.VMEM((16 + width, lanes), jnp.float32),
        ],
        compiler_params=pltpu.CompilerParams(vmem_limit_bytes=40 * 1024 * 1024),
        cost_estimate=pl.CostEstimate(flops=20_000_000_000, bytes_accessed=5_000_000, transcendentals=0),
    )(query_input, key_values, cosine, sine, gain)


def slot_places(route_block, expert_count, capacity):
    flat_routes = route_block.reshape(-1)
    one_hot = (flat_routes[:, None] == jnp.arange(expert_count, dtype=jnp.int32)[None, :]).astype(
        jnp.int32
    )
    earlier = jnp.cumsum(one_hot, axis=0) - one_hot
    return flat_routes * capacity + jnp.sum(earlier * one_hot, axis=1)


def fill_sources(places, token_count, top_count, slot_total):
    source_rows = jnp.full((slot_total,), token_count, jnp.int32)
    pair_rows = jnp.arange(token_count * top_count, dtype=jnp.int32) // top_count
    return source_rows.at[places].set(pair_rows)


def on_device(
    query_input,
    key_input,
    value_input,
    query_gain,
    key_gain,
    mixer_out,
    moe_input,
    moe_gain,
    routes,
    route_weight,
    expert_gate,
    expert_up,
    expert_down,
):
    seq_dev = query_input.shape[0]
    head_width = query_gain.shape[0]
    positions = lax.axis_index("ep") * seq_dev + jnp.arange(seq_dev, dtype=jnp.int32)
    cosine, sine_table = rope_tables(positions, head_width)
    key_value = key_value_rows(
        key_input, value_input, cosine, sine_table, key_gain[:, None]
    )
    incoming = lax.all_gather(key_value, "ep", axis=0, tiled=True)
    attended = flash(query_input, incoming, cosine, sine_table, query_gain[:, None])
    projected = jnp.dot(gather_axes(attended, TP, 1), mixer_out, preferred_element_type=jnp.float32)
    attn_mixed = projected.astype(jnp.bfloat16)
    token_count, model_width = moe_input.shape
    top_count = routes.shape[1]
    local_experts = expert_gate.shape[0]
    senders = lax.axis_size("ep")
    expert_count = local_experts * senders
    capacity = 3 * token_count * top_count // (2 * expert_count)
    features = moe_input.astype(jnp.float32)
    normed = (
        features
        * lax.rsqrt(jnp.mean(features * features, axis=-1, keepdims=True) + epsilon)
        * moe_gain
    ).astype(jnp.bfloat16)
    places = slot_places(routes, expert_count, capacity)
    sources = fill_sources(places, token_count, top_count, expert_count * capacity)
    padded = jnp.concatenate([normed, jnp.zeros((1, model_width), jnp.bfloat16)], axis=0)
    column_width = expert_down.shape[2]
    feature_width = model_width // lax.axis_size(TP)
    own_columns = lax.dynamic_slice_in_dim(
        padded, lax.axis_index(TP) * feature_width, feature_width, 1
    )
    received = lax.all_to_all(own_columns[sources], "ep", split_axis=0, concat_axis=0, tiled=True)
    received = received.reshape(senders, local_experts, capacity, feature_width)
    incoming = lax.all_gather(received, TP, axis=3, tiled=True)
    gate_hidden = jnp.einsum(
        "sjcd,jdf->sjcf", incoming, expert_gate, preferred_element_type=jnp.float32
    )
    up_hidden = jnp.einsum(
        "sjcd,jdf->sjcf", incoming, expert_up, preferred_element_type=jnp.float32
    )
    hidden = (jax.nn.silu(gate_hidden) * up_hidden).astype(jnp.bfloat16)
    expert_out = jnp.einsum(
        "sjcf,jfd->sjcd",
        gathered_copies(hidden, TP, 3),
        expert_down,
        preferred_element_type=jnp.float32,
    )
    expert_out = expert_out.astype(jnp.bfloat16).reshape(
        senders * local_experts * capacity, column_width
    )
    returned = lax.all_to_all(expert_out, "ep", split_axis=0, concat_axis=0, tiled=True)
    picked = returned[places].reshape(token_count, top_count, column_width).astype(jnp.float32)
    shares = route_weight / jnp.sum(route_weight, axis=-1, keepdims=True)
    moe_out = jnp.sum(picked * shares[:, :, None], axis=1).astype(jnp.bfloat16)
    return (attn_mixed, moe_out)


def solution(mesh):
    torus = Mesh(mesh.devices.reshape(mesh.shape["ep"], 4, 4), ("ep", "tp_0", "tp_1"))
    placed = (
        P("ep", TP),
        P("ep", TP),
        P("ep", TP),
        P(),
        P(),
        P(None, TP),
        P("ep", None),
        P(),
        P("ep", None),
        P("ep", None),
        P("ep", None, TP),
        P("ep", None, TP),
        P("ep", None, TP),
    )
    return jax.shard_map(
        on_device,
        mesh=torus,
        in_specs=placed,
        out_specs=(P("ep", TP), P("ep", TP)),
        check_vma=False,
    )
```

```python
import functools

import jax
import jax.numpy as jnp
from jax import lax
from jax.experimental import pallas as pl
from jax.experimental.pallas import tpu as pltpu
from jax.sharding import Mesh
from jax.sharding import PartitionSpec as P

GRID_W = 64
TOP_K = 2
CORES = 2
GROUPS = 4
AXES = ("z", "c", "y", "x")
epsilon = 1e-06
base_theta = 10000.0
log2e = 1.4426950408889634
MESH = pl.DeviceIdType.MESH


def rope_tables(positions, head_width):
    quarter = head_width // 4
    inverse = base_theta ** (-jnp.arange(quarter, dtype=jnp.float32) / quarter)
    grid_row = (positions // GRID_W).astype(jnp.float32)
    grid_col = (positions % GRID_W).astype(jnp.float32)
    angles = jnp.concatenate(
        [inverse[:, None] * grid_row[None, :], inverse[:, None] * grid_col[None, :]], axis=0
    )
    return (jnp.cos(angles), jnp.sin(angles))


def rotated(x, cosine, sine, gain):
    scale = lax.rsqrt(jnp.mean(x * x, axis=0, keepdims=True) + epsilon)
    x = x * scale * gain
    half = x.shape[0] // 2
    first, second = x[:half], x[half:]
    return jnp.concatenate(
        [first * cosine - second * sine, first * sine + second * cosine], axis=0
    )


def ring_offsets(size):
    offsets = [0]
    for step in range(1, size // 2 + 1):
        offsets.append(step)
        if step < size - step:
            offsets.append(-step)
    return offsets


def step_kernel(
    sizes,
    cap,
    q_ref,
    k_ref,
    v_ref,
    cos_ref,
    sin_ref,
    qg_ref,
    kg_ref,
    x_ref,
    xg_ref,
    routes_ref,
    share_ref,
    mixer_hbm,
    gate_hbm,
    up_hbm,
    down_hbm,
    attn_ref,
    moe_ref,
    kv_ref,
    qt_ref,
    s0_ref,
    s1_ref,
    x0_ref,
    x1_ref,
    m_ref,
    o_ref,
    named_ref,
    count_ref,
    weight_ref,
    pick_ref,
    combine_ref,
    chi_ref,
    clo_ref,
    disp_ref,
    rows_ref,
    gu_ref,
    acc_ref,
    hid_ref,
    eo_ref,
    back_ref,
    att_ref,
    mixer_ref,
    gate_ref,
    up_ref,
    down_ref,
    load_sem,
    kv_send,
    kv_recv,
    d_send,
    d_recv,
    r_send,
    r_recv,
    g1_send,
    g1_recv,
    g2_send,
    g2_recv,
    a1_send,
    a1_recv,
    a2_send,
    a2_recv,
    h1_send,
    h1_recv,
    h2_send,
    h2_recv,
):
    Z, Y, X = sizes
    T = Y * X
    experts = Z * CORES
    z, c = lax.axis_index("z"), lax.axis_index("c")
    y, x = lax.axis_index("y"), lax.axis_index("x")
    ep = z * CORES + c
    tp = y * X + x
    offsets = ring_offsets(Z)
    places = [(rel, dc) for rel in offsets for dc in range(CORES)]
    block = 2 * cap
    f32, bf16 = jnp.float32, jnp.bfloat16

    def line(rel, dc):
        return {"z": lax.rem(z + (rel + Z), Z), "c": lax.rem(c + dc, CORES)}

    def x_peer(dx):
        return {"x": lax.rem(x + (dx + X), X)}

    def y_peer(dy):
        return {"y": lax.rem(y + (dy + Y), Y)}

    barrier = pltpu.get_barrier_semaphore()
    greeted = 0
    for rel, dc in places[1:]:
        pl.semaphore_signal(barrier, inc=1, device_id=line(rel, dc), device_id_type=MESH)
        greeted += 1
    for dx in range(1, X):
        pl.semaphore_signal(barrier, inc=1, device_id=x_peer(dx), device_id_type=MESH)
        greeted += 1
    for dy in range(1, Y):
        pl.semaphore_signal(barrier, inc=1, device_id=y_peer(dy), device_id_type=MESH)
        greeted += 1

    loads = [
        pltpu.make_async_copy(gate_hbm, gate_ref, load_sem.at[0]),
        pltpu.make_async_copy(up_hbm, up_ref, load_sem.at[1]),
        pltpu.make_async_copy(down_hbm, down_ref, load_sem.at[2]),
        pltpu.make_async_copy(mixer_hbm, mixer_ref, load_sem.at[3]),
    ]
    for load in loads:
        load.start()

    def remote(src, dst, send, recv, device):
        return pltpu.make_async_remote_copy(
            src_ref=src, dst_ref=dst, send_sem=send, recv_sem=recv, device_id=device, device_id_type=MESH
        )

    rows, features = x_ref.shape
    share = features // T
    half = share // 2
    expert_at = lax.broadcasted_iota(jnp.int32, (experts, rows), 0)
    first = routes_ref[0:1, :] == expert_at
    second = routes_ref[1:2, :] == expert_at
    total_share = share_ref[0:1, :] + share_ref[1:2, :]
    named = jnp.where(first | second, 1.0, 0.0)
    earlier = jnp.where(
        lax.broadcasted_iota(jnp.int32, (rows, rows), 0)
        < lax.broadcasted_iota(jnp.int32, (rows, rows), 1),
        1.0,
        0.0,
    ).astype(bf16)
    count = jnp.dot(named.astype(bf16), earlier, preferred_element_type=f32)
    named_ref[...] = named
    count_ref[...] = jnp.where(named > 0.0, count, -1.0)
    weight_ref[...] = jnp.where(first, share_ref[0:1, :] / total_share, 0.0) + jnp.where(
        second, share_ref[1:2, :] / total_share, 0.0
    )
    slot_at = lax.broadcasted_iota(jnp.int32, (block, rows), 0)
    slot_at = jnp.where(slot_at < cap, slot_at, slot_at - cap).astype(f32)

    @pl.loop(0, experts)
    def _(expert):
        here = count_ref[pl.ds(expert, 1), :] == slot_at
        at = pl.ds(pl.multiple_of(expert * block, block), block)
        pick_ref[at, :] = jnp.where(here, 1.0, 0.0).astype(bf16)
        combine_ref[at, :] = jnp.where(here, weight_ref[pl.ds(expert, 1), :], 0.0)

    chunk = 512
    squares = jnp.zeros((rows, 128), f32)
    for start in range(0, features, chunk):
        part = x_ref[:, start : start + chunk].astype(f32)
        part = part * part
        for lane in range(0, chunk, 128):
            squares = squares + part[:, lane : lane + 128]
    mean = jnp.sum(squares, axis=1, keepdims=True) * (1.0 / features)
    own = pl.ds(pl.multiple_of(tp * share, share), share)
    normed = (x_ref[:, own].astype(f32) * lax.rsqrt(mean + epsilon) * xg_ref[:, own]).astype(bf16)
    picked = jnp.dot(pick_ref[...], normed, preferred_element_type=f32)
    picked = picked.reshape(experts, block, share)
    picked = jnp.concatenate([picked[:, :cap, :half], picked[:, cap:, half:]], axis=1)
    disp_ref[...] = picked.reshape(experts * block, half).astype(bf16)

    width = k_ref.shape[1]
    k_t = rotated(k_ref[...].astype(f32).T, cos_ref[...], sin_ref[...], kg_ref[...])
    kv_ref[0] = jnp.concatenate([k_t.T, v_ref[...].astype(f32)], axis=1).astype(bf16)

    pl.semaphore_wait(barrier, greeted)

    def expert_rows(rel, dc):
        target = line(rel, dc)
        return pl.ds(pl.multiple_of((target["z"] * CORES + target["c"]) * block, block), block)

    def dispatch(p):
        rel, dc = places[p]
        return remote(
            disp_ref.at[expert_rows(-rel, dc)],
            rows_ref.at[y, x, pl.ds(p * block, block)],
            d_send.at[p],
            d_recv.at[p],
            line(-rel, dc),
        )

    kept = pltpu.make_async_copy(
        disp_ref.at[expert_rows(0, 0)], rows_ref.at[y, x, pl.ds(0, block)], d_recv.at[0]
    )
    kept.start()
    for p in range(1, len(places)):
        dispatch(p).start()

    def base(step):
        return 2 + 4 * (step - 1)

    last = Z // 2
    tail = base(last)

    def rightward(step):
        src = lax.select(step == 1, 0, base(step - 1)) if not isinstance(step, int) else (
            0 if step == 1 else base(step - 1)
        )
        return remote(kv_ref.at[src], kv_ref.at[base(step)], kv_send.at[base(step)], kv_recv.at[base(step)], line(1, 0))

    def leftward(step):
        src = lax.select(step == 1, 0, base(step - 1) + 1) if not isinstance(step, int) else (
            0 if step == 1 else base(step - 1) + 1
        )
        to = base(step) + 1
        return remote(kv_ref.at[src], kv_ref.at[to], kv_send.at[to], kv_recv.at[to], line(-1, 0))

    def across(src, to):
        return remote(kv_ref.at[src], kv_ref.at[to], kv_send.at[to], kv_recv.at[to], line(0, 1))

    rightward(1).start()
    leftward(1).start()
    across(0, 1).start()

    tokens = q_ref.shape[0]
    heads = q_ref.shape[1] // width
    lanes = heads * tokens
    q_t = q_ref[...].astype(f32).T
    for head in range(heads):
        turned = rotated(
            q_t[head * width : (head + 1) * width], cos_ref[...], sin_ref[...], qg_ref[...]
        )
        turned = turned.astype(bf16).astype(f32) * (width ** (-0.5))
        qt_ref[:width, head * tokens : (head + 1) * tokens] = turned.astype(bf16)
    qt_ref[width:, :] = jnp.zeros((width, lanes), bf16)
    m_ref[...] = jnp.full(m_ref.shape, -1e30, f32)
    o_ref[...] = jnp.zeros(o_ref.shape, f32)
    s_ref, mx_ref = (s0_ref, s1_ref), (x0_ref, x1_ref)

    def scores(slot, buffer):
        s = jnp.dot(kv_ref[slot], qt_ref[...], preferred_element_type=f32)
        s_ref[buffer][...] = s
        mx_ref[buffer][...] = jnp.max(s.reshape(tokens // 8, 8, lanes), axis=0)

    def absorb(slot, buffer):
        old = m_ref[...]
        new = jnp.maximum(old, jnp.max(mx_ref[buffer][...], axis=0, keepdims=True) * log2e)
        m_ref[...] = new
        factor = jnp.exp2(old - new)
        p = jnp.exp2(s_ref[buffer][...] * log2e - new[:1]).astype(bf16)
        v_t = kv_ref[slot].T[width:]
        lhs = jnp.concatenate([jnp.ones((16, tokens), bf16), v_t], axis=0)
        part = jnp.dot(lhs, p, preferred_element_type=f32)
        o_ref[...] = o_ref[...] * factor[:1] + part

    def along_x(ref, piece, send, recv, n):
        return [
            (
                remote(ref.at[y, x, piece], ref.at[y, x, piece], send.at[n, dx - 1], recv.at[n, dx - 1], x_peer(dx)),
                remote(
                    ref.at[y, x_peer(-dx)["x"], piece],
                    ref.at[y, x_peer(-dx)["x"], piece],
                    send.at[n, dx - 1],
                    recv.at[n, dx - 1],
                    x_peer(dx),
                ),
            )
            for dx in range(1, X)
        ]

    def along_y(ref, piece, send, recv, n):
        return [
            (
                remote(ref.at[y, x, piece], ref.at[y, x, piece], send.at[n, dy - 1], recv.at[n, dy - 1], y_peer(dy)),
                remote(
                    ref.at[y_peer(-dy)["y"], x, piece],
                    ref.at[y_peer(-dy)["y"], x, piece],
                    send.at[n, dy - 1],
                    recv.at[n, dy - 1],
                    y_peer(dy),
                ),
            )
            for dy in range(1, Y)
        ]

    def then_y(ref, piece, send, recv, n):
        every = pl.ds(0, X)
        return [
            (
                remote(ref.at[y, every, piece], ref.at[y, every, piece], send.at[n, dy - 1], recv.at[n, dy - 1], y_peer(dy)),
                remote(
                    ref.at[y_peer(-dy)["y"], every, piece],
                    ref.at[y_peer(-dy)["y"], every, piece],
                    send.at[n, dy - 1],
                    recv.at[n, dy - 1],
                    y_peer(dy),
                ),
            )
            for dy in range(1, Y)
        ]

    def then_x(ref, piece, send, recv, n):
        every = pl.ds(0, Y)
        return [
            (
                remote(ref.at[every, x, piece], ref.at[every, x, piece], send.at[n, dx - 1], recv.at[n, dx - 1], x_peer(dx)),
                remote(
                    ref.at[every, x_peer(-dx)["x"], piece],
                    ref.at[every, x_peer(-dx)["x"], piece],
                    send.at[n, dx - 1],
                    recv.at[n, dx - 1],
                    x_peer(dx),
                ),
            )
            for dx in range(1, X)
        ]

    def hops(ref, piece, n, send1, recv1, send2, recv2):
        if n % 2 == 0:
            return along_x(ref, piece, send1, recv1, n), then_y(ref, piece, send2, recv2, n)
        return along_y(ref, piece, send1, recv1, n), then_x(ref, piece, send2, recv2, n)

    def start(copies):
        for out, _ in copies:
            out.start()

    def arrive(copies):
        for _, into in copies:
            into.wait_recv()

    def sent(copies):
        for out, _ in copies:
            out.wait_send()

    per_group = len(places) // GROUPS
    span = per_group * block

    def rows_hops(group):
        return hops(rows_ref, pl.ds(group * span, span), group, g1_send, g1_recv, g2_send, g2_recv)

    def group_arrived(group):
        for p in range(group * per_group, (group + 1) * per_group):
            if p == 0:
                kept.wait()
            else:
                dispatch(p).wait_recv()
        start(rows_hops(group)[0])

    def group_forwarded(group):
        first_hop, second_hop = rows_hops(group)
        arrive(first_hop)
        start(second_hop)

    scores(0, 0)
    across(0, 1).wait_recv()
    scores(1, 1)
    absorb(0, 0)

    for load in loads:
        load.wait()
    for t in range(T):
        top, low = t * share, t * share + half
        gu_ref[t * half : (t + 1) * half, :] = jnp.concatenate(
            [
                gate_ref[top : top + half, :],
                up_ref[top : top + half, :],
                gate_ref[low : low + half, :],
                up_ref[low : low + half, :],
            ],
            axis=1,
        )
    for e in range(0, experts * block, 256):
        turned = combine_ref[e : e + 256, :].T
        high = turned.astype(bf16)
        chi_ref[:, e : e + 256] = high
        clo_ref[:, e : e + 256] = (turned - high.astype(f32)).astype(bf16)

    @pl.loop(1, last)
    def _(step):
        at = base(step)
        rightward(step).wait_recv()
        rightward(step + 1).start()
        across(at, at + 2).start()
        leftward(step).wait_recv()

        @pl.when(step < last - 1)
        def _():
            leftward(step + 1).start()

        across(at + 1, at + 3).start()
        for group in range(GROUPS):

            @pl.when(step == min(group + 1, last - 1))
            def _(group=group):
                group_arrived(group)

            @pl.when(step == min(group + 2, last - 1))
            def _(group=group):
                group_forwarded(group)

        @pl.loop(0, 2)
        def _(pair):
            even = at + 2 * pair

            @pl.when(pair == 1)
            def _():
                across(at, at + 2).wait_recv()
                across(at + 1, at + 3).wait_recv()

            scores(even, 0)
            absorb(even - 1, 1)
            scores(even + 1, 1)
            absorb(even, 0)

    rightward(last).wait_recv()
    across(tail, tail + 1).start()
    scores(tail, 0)
    absorb(tail - 1, 1)
    across(tail, tail + 1).wait_recv()
    scores(tail + 1, 1)
    absorb(tail, 0)
    absorb(tail + 1, 1)

    attended = o_ref[16:, :] / o_ref[:1, :]
    for head in range(heads):
        piece = attended[:, head * tokens : (head + 1) * tokens].T
        att_ref[y, x, :, head * width : (head + 1) * width] = piece.astype(bf16)
    att_half = tokens // 2
    att_hops = [
        hops(att_ref, pl.ds(n * att_half, att_half), n, a1_send, a1_recv, a2_send, a2_recv)
        for n in range(2)
    ]
    for n in range(2):
        start(att_hops[n][0])

    hidden_width = gate_ref.shape[1]
    pack = per_group * cap // 2
    for group in range(GROUPS):
        arrive(rows_hops(group)[1])
        at = pl.ds(group * span, span)
        total = None
        for t in range(0, T, min(T, 4)):
            many = range(t, min(t + 4, T))
            lhs = jnp.concatenate([rows_ref[u // X, u % X, at, :] for u in many], axis=1)
            term = jnp.dot(
                lhs, gu_ref[t * half : (t + len(many)) * half, :], preferred_element_type=f32
            )
            total = term if total is None else total + term
        both = total.reshape(per_group, block, 4 * hidden_width)
        both = both[:, :cap, : 2 * hidden_width] + both[:, cap:, 2 * hidden_width :]
        both = both.reshape(per_group * cap, 2 * hidden_width)
        gate = both[:, :hidden_width]
        up = both[:, hidden_width:]
        hidden = gate / (1.0 + jnp.exp(-gate)) * up
        hidden = jnp.concatenate([hidden[:pack], hidden[pack:]], axis=1)
        hid_ref[y, x, group * pack : (group + 1) * pack, :] = hidden.astype(bf16)
    hid_half = GROUPS * pack // 2
    hid_hops = [
        hops(hid_ref, pl.ds(n * hid_half, hid_half), n, h1_send, h1_recv, h2_send, h2_recv)
        for n in range(2)
    ]
    for n in range(2):
        start(hid_hops[n][0])
    for n in range(2):
        arrive(hid_hops[n][0])
        start(hid_hops[n][1])
    for n in range(2):
        arrive(att_hops[n][0])
        start(att_hops[n][1])

    def giveback(p):
        rel, dc = places[p]
        mine = pl.ds(pl.multiple_of(ep * block, block), block)
        return remote(
            eo_ref.at[pl.ds(p * block, block)], back_ref.at[mine], r_send.at[p], r_recv.at[p], line(rel, dc)
        )

    def returned(p):
        rel, dc = places[p]
        at = expert_rows(-rel, dc)
        return remote(back_ref.at[at], back_ref.at[at], r_send.at[p], r_recv.at[p], line(rel, dc))

    mine = pl.ds(pl.multiple_of(ep * block, block), block)
    own_back = pltpu.make_async_copy(eo_ref.at[pl.ds(0, block)], back_ref.at[mine], r_recv.at[0])
    for n in range(2):
        arrive(hid_hops[n][1])
        for group in range(n * GROUPS // 2, (n + 1) * GROUPS // 2):
            lo = jnp.concatenate(
                [hid_ref[u // X, u % X, group * pack : (group + 1) * pack, :hidden_width] for u in range(T)],
                axis=1,
            )
            hi = jnp.concatenate(
                [hid_ref[u // X, u % X, group * pack : (group + 1) * pack, hidden_width:] for u in range(T)],
                axis=1,
            )
            out = jnp.dot(
                jnp.concatenate([lo, hi], axis=0), down_ref[...], preferred_element_type=f32
            )
            out = out.reshape(per_group, cap, share)
            out = jnp.concatenate([out[:, :, :half], out[:, :, half:]], axis=1)
            eo_ref[group * span : (group + 1) * span, :] = out.reshape(span, half).astype(bf16)
            for p in range(group * per_group, (group + 1) * per_group):
                if p == 0:
                    own_back.start()
                else:
                    giveback(p).start()

    for n in range(2):
        arrive(att_hops[n][1])
        at = pl.ds(n * att_half, att_half)
        lhs = jnp.concatenate([att_ref[u // X, u % X, at, :] for u in range(T)], axis=1)
        attn_ref[n * att_half : (n + 1) * att_half, :] = jnp.dot(
            lhs, mixer_ref[...], preferred_element_type=f32
        ).astype(bf16)

    own_back.wait()
    for p in range(1, len(places)):
        returned(p).wait_recv()
    back = back_ref[...].astype(f32).reshape(experts, block, half)
    blank = jnp.zeros((experts, cap, half), f32)
    wide = jnp.concatenate(
        [
            jnp.concatenate([back[:, :cap], blank], axis=1),
            jnp.concatenate([blank, back[:, cap:]], axis=1),
        ],
        axis=2,
    )
    wide = wide.reshape(experts * block, share).astype(bf16)
    moe = jnp.dot(chi_ref[...], wide, preferred_element_type=f32)
    moe = moe + jnp.dot(clo_ref[...], wide, preferred_element_type=f32)
    moe_ref[...] = moe.astype(bf16)

    across(0, 1).wait_send()
    for step in range(1, last + 1):
        rightward(step).wait_send()
        if step < last:
            leftward(step).wait_send()
            across(base(step), base(step) + 2).wait_send()
            across(base(step) + 1, base(step) + 3).wait_send()
    across(tail, tail + 1).wait_send()
    for p in range(1, len(places)):
        dispatch(p).wait_send()
        giveback(p).wait_send()
    for group in range(GROUPS):
        for copies in rows_hops(group):
            sent(copies)
    for n in range(2):
        for copies in att_hops[n] + hid_hops[n]:
            sent(copies)


def on_device(
    sizes,
    query_input,
    key_input,
    value_input,
    query_gain,
    key_gain,
    mixer_out,
    moe_input,
    moe_gain,
    routes,
    route_weight,
    expert_gate,
    expert_up,
    expert_down,
):
    Z, Y, X = sizes
    T = Y * X
    experts = Z * CORES
    tokens, columns = query_input.shape
    width = query_gain.shape[0]
    lanes = tokens * (columns // width)
    ep = lax.axis_index("z") * CORES + lax.axis_index("c")
    positions = ep * tokens + jnp.arange(tokens, dtype=jnp.int32)
    cosine, sine = rope_tables(positions, width)
    rows, features = moe_input.shape
    share = features // T
    half = share // 2
    cap = 3 * rows * TOP_K // (2 * experts)
    block = 2 * cap
    hidden = expert_gate.shape[2]
    gate, up, down = expert_gate[0], expert_up[0], expert_down[0]
    vmem = pl.BlockSpec(memory_space=pltpu.VMEM)
    hbm = pl.BlockSpec(memory_space=pl.ANY)
    bf16, f32 = jnp.bfloat16, jnp.float32
    dma = pltpu.SemaphoreType.DMA
    last = Z // 2
    slots = experts
    total = experts * block
    pieces = ((GROUPS, X - 1), (GROUPS, Y - 1))
    wide = max(X, Y) - 1
    return pl.pallas_call(
        functools.partial(step_kernel, sizes, cap),
        out_shape=(
            jax.ShapeDtypeStruct((tokens, mixer_out.shape[1]), bf16),
            jax.ShapeDtypeStruct((rows, share), bf16),
        ),
        in_specs=[vmem] * 11 + [hbm] * 4,
        out_specs=(vmem, vmem),
        scratch_shapes=[
            pltpu.VMEM((slots, tokens, 2 * width), bf16),
            pltpu.VMEM((2 * width, lanes), bf16),
            pltpu.VMEM((tokens, lanes), f32),
            pltpu.VMEM((tokens, lanes), f32),
            pltpu.VMEM((8, lanes), f32),
            pltpu.VMEM((8, lanes), f32),
            pltpu.VMEM((8, lanes), f32),
            pltpu.VMEM((16 + width, lanes), f32),
            pltpu.VMEM((experts, rows), f32),
            pltpu.VMEM((experts, rows), f32),
            pltpu.VMEM((experts, rows), f32),
            pltpu.VMEM((total, rows), bf16),
            pltpu.VMEM((total, rows), f32),
            pltpu.VMEM((rows, total), bf16),
            pltpu.VMEM((rows, total), bf16),
            pltpu.VMEM((total, half), bf16),
            pltpu.VMEM((Y, X, total, half), bf16),
            pltpu.VMEM((T * half, 4 * hidden), bf16),
            pltpu.VMEM((8, 128), f32),
            pltpu.VMEM((Y, X, total // 4, 2 * hidden), bf16),
            pltpu.VMEM((total, half), bf16),
            pltpu.VMEM((total, half), bf16),
            pltpu.VMEM((Y, X, tokens, columns), bf16),
            pltpu.VMEM(mixer_out.shape, bf16),
            pltpu.VMEM(gate.shape, bf16),
            pltpu.VMEM(up.shape, bf16),
            pltpu.VMEM(down.shape, bf16),
            dma((4,)),
            dma((slots,)),
            dma((slots,)),
            dma((experts,)),
            dma((experts,)),
            dma((experts,)),
            dma((experts,)),
        ]
        + [dma((GROUPS, wide))] * 4
        + [dma((2, wide))] * 8,
        compiler_params=pltpu.CompilerParams(
            collective_id=0, has_side_effects=True, vmem_limit_bytes=60 * 1024 * 1024
        ),
    )(
        query_input,
        key_input,
        value_input,
        cosine,
        sine,
        query_gain[:, None],
        key_gain[:, None],
        moe_input,
        moe_gain[None, :],
        routes.T,
        route_weight.T,
        mixer_out,
        gate,
        up,
        down,
    )


def solution(mesh, grid=None):
    n_ep, n_tp = mesh.shape["ep"], mesh.shape["tp"]
    sizes = grid or (n_ep // CORES, 4, n_tp // 4)
    Z, Y, X = sizes
    torus = Mesh(mesh.devices.reshape(Z, CORES, Y, X), AXES)
    ep, tp = ("z", "c"), ("y", "x")
    placed = (
        P(ep, tp),
        P(ep, tp),
        P(ep, tp),
        P(),
        P(),
        P(None, tp),
        P(ep, None),
        P(),
        P(ep, None),
        P(ep, None),
        P(ep, None, tp),
        P(ep, None, tp),
        P(ep, None, tp),
    )
    return jax.shard_map(
        functools.partial(on_device, sizes),
        mesh=torus,
        in_specs=placed,
        out_specs=(P(ep, tp), P(ep, tp)),
        check_vma=False,
    )
```

```python
import functools

import jax
import jax.numpy as jnp
from jax import lax
from jax.experimental import pallas as pl
from jax.experimental.pallas import tpu as pltpu
from jax.sharding import Mesh
from jax.sharding import PartitionSpec as P

GRID_W = 64
TOP_K = 2
CORES = 2
AXES = ("z", "c", "y", "x")
epsilon = 1e-06
base_theta = 10000.0
log2e = 1.4426950408889634
MESH = pl.DeviceIdType.MESH


def rope_tables(positions, head_width):
    quarter = head_width // 4
    inverse = base_theta ** (-jnp.arange(quarter, dtype=jnp.float32) / quarter)
    grid_row = (positions // GRID_W).astype(jnp.float32)
    grid_col = (positions % GRID_W).astype(jnp.float32)
    angles = jnp.concatenate(
        [inverse[:, None] * grid_row[None, :], inverse[:, None] * grid_col[None, :]], axis=0
    )
    return (jnp.cos(angles), jnp.sin(angles))


def rotated(x, cosine, sine, gain):
    scale = lax.rsqrt(jnp.mean(x * x, axis=0, keepdims=True) + epsilon)
    x = x * scale * gain
    half = x.shape[0] // 2
    first, second = x[:half], x[half:]
    return jnp.concatenate(
        [first * cosine - second * sine, first * sine + second * cosine], axis=0
    )


def ring_offsets(size):
    offsets = [0]
    for step in range(1, size // 2 + 1):
        offsets.append(step)
        if step < size - step:
            offsets.append(-step)
    return offsets


def step_kernel(
    sizes,
    cap,
    q_hbm,
    k_hbm,
    v_hbm,
    cos_hbm,
    sin_hbm,
    qg_hbm,
    kg_hbm,
    x_hbm,
    xg_hbm,
    routes_hbm,
    share_hbm,
    mixer_hbm,
    gate_hbm,
    up_hbm,
    down_hbm,
    attn_hbm,
    moe_hbm,
    q_ref,
    k_ref,
    v_ref,
    cos_ref,
    sin_ref,
    qg_ref,
    kg_ref,
    x_ref,
    xg_ref,
    routes_ref,
    share_ref,
    mixer_ref,
    gate_ref,
    up_ref,
    down_ref,
    attn_ref,
    moe_ref,
    kv_ref,
    qt_ref,
    s0_ref,
    s1_ref,
    x0_ref,
    x1_ref,
    m_ref,
    o_ref,
    count_ref,
    weight_ref,
    pick_ref,
    combine_ref,
    chi_ref,
    clo_ref,
    disp_ref,
    rows_ref,
    gu_ref,
    hid_ref,
    eo_ref,
    back_ref,
    att_ref,
    load_sem,
    store_sem,
    kv_send,
    kv_recv,
    d_send,
    d_recv,
    r_send,
    r_recv,
    g_send,
    g_recv,
):
    Z, Y, X = sizes
    T = Y * X
    experts = Z * CORES
    z, c = lax.axis_index("z"), lax.axis_index("c")
    y, x = lax.axis_index("y"), lax.axis_index("x")
    ep = z * CORES + c
    tp = y * X + x
    offsets = ring_offsets(Z)
    places = [(rel, dc) for rel in offsets for dc in range(CORES)]
    block = 2 * cap
    f32, bf16 = jnp.float32, jnp.bfloat16

    def line(rel, dc):
        return {"z": lax.rem(z + (rel + Z), Z), "c": lax.rem(c + dc, CORES)}

    barrier = pltpu.get_barrier_semaphore()
    greeted = 0
    for rel, dc in reversed(places[1:]):
        pl.semaphore_signal(barrier, inc=1, device_id=line(rel, dc), device_id_type=MESH)
        greeted += 1
    for axis, at, size in (("x", x, X), ("y", y, Y)):
        for step in (1, size - 1) if size > 1 else ():
            device = {axis: lax.rem(at + step, size)}
            pl.semaphore_signal(barrier, inc=1, device_id=device, device_id_type=MESH)
            greeted += 1

    pairs = (
        (x_hbm, x_ref),
        (routes_hbm, routes_ref),
        (share_hbm, share_ref),
        (xg_hbm, xg_ref),
        (k_hbm, k_ref),
        (v_hbm, v_ref),
        (cos_hbm, cos_ref),
        (sin_hbm, sin_ref),
        (kg_hbm, kg_ref),
        (q_hbm, q_ref),
        (qg_hbm, qg_ref),
        (gate_hbm, gate_ref),
        (up_hbm, up_ref),
        (down_hbm, down_ref),
        (mixer_hbm, mixer_ref),
    )
    loads = [
        pltpu.make_async_copy(src, dst, load_sem.at[n]) for n, (src, dst) in enumerate(pairs)
    ]
    for load in loads:
        load.start()

    def remote(src, dst, send, recv, device):
        return pltpu.make_async_remote_copy(
            src_ref=src, dst_ref=dst, send_sem=send, recv_sem=recv, device_id=device, device_id_type=MESH
        )

    def column(row):
        return jnp.broadcast_to(row, (8, row.shape[1])).T[:, :1]

    rows, features = x_ref.shape
    share = features // T
    half = share // 2
    for load in loads[1:3]:
        load.wait()
    expert_at = lax.broadcasted_iota(jnp.int32, (experts, rows), 0)
    first = routes_ref[0:1, :] == expert_at
    second = routes_ref[1:2, :] == expert_at
    total_share = share_ref[0:1, :] + share_ref[1:2, :]
    named = jnp.where(first | second, 1.0, 0.0)
    earlier = jnp.where(
        lax.broadcasted_iota(jnp.int32, (rows, rows), 0)
        < lax.broadcasted_iota(jnp.int32, (rows, rows), 1),
        1.0,
        0.0,
    ).astype(bf16)
    count = jnp.dot(named.astype(bf16), earlier, preferred_element_type=f32)
    count_ref[...] = jnp.where(named > 0.0, count, -1.0)
    weight_ref[...] = jnp.where(first, share_ref[0:1, :] / total_share, 0.0) + jnp.where(
        second, share_ref[1:2, :] / total_share, 0.0
    )
    slot_at = lax.broadcasted_iota(jnp.int32, (block, rows), 0)
    slot_at = jnp.where(slot_at < cap, slot_at, slot_at - cap).astype(f32)

    @pl.loop(0, experts)
    def _(expert):
        here = count_ref[pl.ds(expert, 1), :] == slot_at
        at = pl.ds(pl.multiple_of(expert * block, block), block)
        pick_ref[at, :] = jnp.where(here, 1.0, 0.0).astype(bf16)
        combine_ref[at, :] = jnp.where(here, weight_ref[pl.ds(expert, 1), :], 0.0)

    loads[0].wait()
    loads[3].wait()
    chunk = 512
    squares = jnp.zeros((rows, 128), f32)
    for start in range(0, features, chunk):
        part = x_ref[:, start : start + chunk].astype(f32)
        part = part * part
        for lane in range(0, chunk, 128):
            squares = squares + part[:, lane : lane + 128]
    mean = jnp.sum(squares, axis=1, keepdims=True) * (1.0 / features)
    own = pl.ds(pl.multiple_of(tp * share, share), share)
    normed = (x_ref[:, own].astype(f32) * lax.rsqrt(mean + epsilon) * xg_ref[:, own]).astype(bf16)
    picked = jnp.dot(pick_ref[...], normed, preferred_element_type=f32)
    picked = picked.reshape(experts, block, share)
    picked = jnp.concatenate([picked[:, :cap, :half], picked[:, cap:, half:]], axis=1)
    disp_ref[...] = picked.reshape(experts * block, half).astype(bf16)

    for load in loads[4:]:
        load.wait()
    width = k_ref.shape[0]
    k_t = rotated(k_ref[...].astype(f32), cos_ref[...], sin_ref[...], column(kg_ref[...]))
    kv_ref[0] = jnp.concatenate([k_t, v_ref[...].astype(f32)], axis=0).T.astype(bf16)

    tokens = q_ref.shape[0]
    heads = q_ref.shape[1] // width
    lanes = heads * tokens
    q_t = q_ref[...].astype(f32).T
    q_gain = column(qg_ref[...])
    for head in range(heads):
        turned = rotated(
            q_t[head * width : (head + 1) * width], cos_ref[...], sin_ref[...], q_gain
        )
        turned = turned.astype(bf16).astype(f32) * (width ** (-0.5))
        qt_ref[:width, head * tokens : (head + 1) * tokens] = turned.astype(bf16)
    qt_ref[width:, :] = jnp.zeros((width, lanes), bf16)
    m_ref[...] = jnp.full(m_ref.shape, -1e30, f32)
    o_ref[...] = jnp.zeros(o_ref.shape, f32)

    hidden_width = gate_ref.shape[0]
    for t in range(T):
        top, low, to = t * share, t * share + half, t * half
        gu_ref[:, to : to + half] = jnp.concatenate(
            [
                gate_ref[:, top : top + half],
                up_ref[:, top : top + half],
                gate_ref[:, low : low + half],
                up_ref[:, low : low + half],
            ],
            axis=0,
        )
    for e in range(0, experts * block, 256):
        turned = combine_ref[e : e + 256, :].T
        high = turned.astype(bf16)
        chi_ref[:, e : e + 256] = high
        clo_ref[:, e : e + 256] = (turned - high.astype(f32)).astype(bf16)

    pl.semaphore_wait(barrier, greeted)

    def expert_rows(rel, dc):
        target = line(rel, dc)
        return pl.ds(pl.multiple_of((target["z"] * CORES + target["c"]) * block, block), block)

    def dispatch(p):
        rel, dc = places[p]
        return remote(
            disp_ref.at[expert_rows(-rel, dc)],
            rows_ref.at[y, x, pl.ds(p * block, block)],
            d_send.at[p],
            d_recv.at[p],
            line(-rel, dc),
        )

    kept = pltpu.make_async_copy(
        disp_ref.at[expert_rows(0, 0)], rows_ref.at[y, x, pl.ds(0, block)], d_recv.at[0]
    )
    kept.start()
    for p in range(1, len(places)):
        dispatch(p).start()

    def base(step):
        return 2 + 4 * (step - 1)

    last = Z // 2
    tail = base(last)

    def before(step):
        if isinstance(step, int):
            return 0 if step == 1 else base(step - 1)
        return lax.select(step == 1, 0, base(step - 1))

    def before_left(step):
        if isinstance(step, int):
            return 0 if step == 1 else base(step - 1) + 1
        return lax.select(step == 1, 0, base(step - 1) + 1)

    def moved(src, to, device):
        return remote(kv_ref.at[src], kv_ref.at[to], kv_send.at[to], kv_recv.at[to], device)

    def rightward(step):
        return moved(before(step), base(step), line(1, 0))

    def leftward(step):
        return moved(before_left(step), base(step) + 1, line(-1, 0))

    def across(src, to):
        return moved(src, to, line(0, 1))

    rightward(1).start()
    leftward(1).start()
    across(0, 1).start()
    s_ref, mx_ref = (s0_ref, s1_ref), (x0_ref, x1_ref)

    def scores(slot, buffer):
        s = jnp.dot(kv_ref[slot], qt_ref[...], preferred_element_type=f32)
        s_ref[buffer][...] = s
        mx_ref[buffer][...] = jnp.max(s.reshape(tokens // 8, 8, lanes), axis=0)

    def absorb(slot, buffer):
        old = m_ref[...]
        new = jnp.maximum(old, jnp.max(mx_ref[buffer][...], axis=0, keepdims=True) * log2e)
        m_ref[...] = new
        factor = jnp.exp2(old - new)
        p = jnp.exp2(s_ref[buffer][...] * log2e - new[:1]).astype(bf16)
        v_t = kv_ref[slot].T[width:]
        lhs = jnp.concatenate([jnp.ones((16, tokens), bf16), v_t], axis=0)
        part = jnp.dot(lhs, p, preferred_element_type=f32)
        o_ref[...] = o_ref[...] * factor[:1] + part

    def stage_copies(ref, begin, length, x_first, stage, n):
        moving_x = x_first == (stage < 2)
        at, size = (x, X) if moving_x else (y, Y)
        if size == 1:
            return []
        found = []
        for way, step in enumerate((1, -1)):
            behind = lax.rem(at - step + size, size)
            opposite = lax.rem(at + 2, size)
            device = {"x" if moving_x else "y": lax.rem(at + step + size, size)}
            if stage % 2 == 0:
                piece = pl.ds(begin, length)
                out_at, in_at = at, behind
            else:
                piece = pl.ds(begin + way * (length // 2), length // 2)
                out_at, in_at = behind, opposite
            every = pl.ds(0, Y if moving_x else X)

            def view(index):
                if stage < 2:
                    where = (y, index) if moving_x else (index, x)
                else:
                    where = (every, index) if moving_x else (index, every)
                return ref.at[where[0], where[1], piece]

            send, recv = g_send.at[n, stage, way], g_recv.at[n, stage, way]
            found.append((view(out_at), view(in_at), send, recv, device))
        return found

    def gather_stage(which, stage):
        ref, pieces, n = which
        found = []
        for number, (begin, length) in enumerate(pieces):
            found += stage_copies(ref, begin, length, number % 2 == 0, stage, n + number)
        return found

    def go(which, stage):
        for out, _, send, recv, device in gather_stage(which, stage):
            remote(out, out, send, recv, device).start()

    def come(which, stage):
        for _, into, send, recv, device in gather_stage(which, stage):
            remote(into, into, send, recv, device).wait_recv()

    def gone(which):
        for stage in range(4):
            for out, _, send, recv, device in gather_stage(which, stage):
                remote(out, out, send, recv, device).wait_send()

    def onward(which, stage):
        come(which, stage)
        go(which, stage + 1)

    groups = 4
    per_group = len(places) // groups
    span = per_group * block
    pack = per_group * cap // 2
    att_half = tokens // 2
    routed = [
        (rows_ref, [(g * span, span) for g in (2 * m, 2 * m + 1)], 2 * m) for m in range(2)
    ]
    hidden_units = [
        (hid_ref, [(g * pack, pack) for g in (2 * m, 2 * m + 1)], 4 + 2 * m) for m in range(2)
    ]
    attended_all = (att_ref, [(0, att_half), (att_half, att_half)], 8)

    def dispatched(m):
        for p in range(2 * m * per_group, 2 * (m + 1) * per_group):
            if p == 0:
                kept.wait()
            else:
                dispatch(p).wait_recv()
        go(routed[m], 0)

    def gate_up(m):
        for group in (2 * m, 2 * m + 1):
            at = pl.ds(group * span, span)
            total = None
            for t in range(0, T, min(T, 4)):
                many = range(t, min(t + 4, T))
                lhs = jnp.concatenate([rows_ref[u // X, u % X, at, :] for u in many], axis=1)
                term = lax.dot_general(
                    lhs,
                    gu_ref[:, t * half : (t + len(many)) * half],
                    (((1,), (1,)), ((), ())),
                    preferred_element_type=f32,
                )
                total = term if total is None else total + term
            both = total.reshape(per_group, block, 4 * hidden_width)
            both = both[:, :cap, : 2 * hidden_width] + both[:, cap:, 2 * hidden_width :]
            both = both.reshape(per_group * cap, 2 * hidden_width)
            gate = both[:, :hidden_width]
            up = both[:, hidden_width:]
            hidden = gate / (1.0 + jnp.exp(-gate)) * up
            hidden = jnp.concatenate([hidden[:pack], hidden[pack:]], axis=1)
            hid_ref[y, x, group * pack : (group + 1) * pack, :] = hidden.astype(bf16)
        go(hidden_units[m], 0)

    def giveback(p):
        rel, dc = places[p]
        mine = pl.ds(pl.multiple_of(ep * block, block), block)
        return remote(
            eo_ref.at[pl.ds(p * block, block)], back_ref.at[mine], r_send.at[p], r_recv.at[p], line(rel, dc)
        )

    def returned(p):
        rel, dc = places[p]
        at = expert_rows(-rel, dc)
        return remote(back_ref.at[at], back_ref.at[at], r_send.at[p], r_recv.at[p], line(rel, dc))

    own_back = pltpu.make_async_copy(
        eo_ref.at[pl.ds(0, block)],
        back_ref.at[pl.ds(pl.multiple_of(ep * block, block), block)],
        r_recv.at[0],
    )

    def down(m):
        for group in (2 * m, 2 * m + 1):
            at = slice(group * pack, (group + 1) * pack)
            lo = jnp.concatenate(
                [hid_ref[u // X, u % X, at, :hidden_width] for u in range(T)], axis=1
            )
            hi = jnp.concatenate(
                [hid_ref[u // X, u % X, at, hidden_width:] for u in range(T)], axis=1
            )
            out = jnp.dot(
                jnp.concatenate([lo, hi], axis=0), down_ref[...], preferred_element_type=f32
            )
            out = out.reshape(per_group, cap, share)
            out = jnp.concatenate([out[:, :, :half], out[:, :, half:]], axis=1)
            eo_ref[group * span : (group + 1) * span, :] = out.reshape(span, half).astype(bf16)
            for p in range(group * per_group, (group + 1) * per_group):
                if p == 0:
                    own_back.start()
                else:
                    giveback(p).start()

    def attended_out():
        attended = o_ref[16:, :] / o_ref[:1, :]
        for head in range(heads):
            piece = attended[:, head * tokens : (head + 1) * tokens].T
            att_ref[y, x, :, head * width : (head + 1) * width] = piece.astype(bf16)
        go(attended_all, 0)

    scores(0, 0)
    across(0, 1).wait_recv()
    scores(1, 1)
    absorb(0, 0)

    events = {
        0: [
            ("D0", lambda: dispatched(0)),
            ("G01", lambda: onward(routed[0], 0)),
            ("G02", lambda: onward(routed[0], 1)),
            ("G03", lambda: onward(routed[0], 2)),
            ("D1", lambda: dispatched(1)),
        ],
        2: [("G11", lambda: onward(routed[1], 0))],
        3: [
            ("G12", lambda: onward(routed[1], 1)),
            ("G04", lambda: come(routed[0], 3)),
            ("GU0", lambda: gate_up(0)),
        ],
        5: [("G13", lambda: onward(routed[1], 2)), ("H01", lambda: onward(hidden_units[0], 0))],
        6: [("H02", lambda: onward(hidden_units[0], 1))],
        7: [
            ("G14", lambda: come(routed[1], 3)),
            ("GU1", lambda: gate_up(1)),
            ("H03", lambda: onward(hidden_units[0], 2)),
        ],
        8: [
            ("H11", lambda: onward(hidden_units[1], 0)),
            ("H04", lambda: come(hidden_units[0], 3)),
            ("DN0", lambda: down(0)),
        ],
        9: [
            ("ATT", attended_out),
            ("H12", lambda: onward(hidden_units[1], 1)),
            ("A1", lambda: onward(attended_all, 0)),
            ("H13", lambda: onward(hidden_units[1], 2)),
            ("A2", lambda: onward(attended_all, 1)),
            ("H14", lambda: come(hidden_units[1], 3)),
            ("DN1", lambda: down(1)),
            ("A3", lambda: onward(attended_all, 2)),
            ("A4", lambda: come(attended_all, 3)),
        ],
    }

    def run(number):
        for name, event in events.get(number, ()):
            event()

    by_step = {}
    for number in sorted(events):
        by_step.setdefault(number if number in (0, 9) else min(max(number, 1), last), []).append(number)

    run(0)

    @pl.loop(1, last)
    def _(step):
        at = base(step)
        rightward(step).wait_recv()
        rightward(step + 1).start()
        across(at, at + 2).start()
        leftward(step).wait_recv()

        @pl.when(step < last - 1)
        def _():
            leftward(step + 1).start()

        across(at + 1, at + 3).start()
        for number in range(1, last):
            if number in by_step:

                @pl.when(step == number)
                def _(number=number):
                    for event in by_step[number]:
                        run(event)

        @pl.loop(0, 2)
        def _(pair):
            even = at + 2 * pair


            @pl.when(pair == 1)
            def _():
                across(at, at + 2).wait_recv()
                across(at + 1, at + 3).wait_recv()

            scores(even, 0)
            absorb(even - 1, 1)
            scores(even + 1, 1)
            absorb(even, 0)

    rightward(last).wait_recv()
    across(tail, tail + 1).start()
    for event in by_step.get(last, ()):
        run(event)
    scores(tail, 0)
    absorb(tail - 1, 1)
    across(tail, tail + 1).wait_recv()
    scores(tail + 1, 1)
    absorb(tail, 0)
    absorb(tail + 1, 1)
    run(9)

    lhs = jnp.concatenate([att_ref[u // X, u % X] for u in range(T)], axis=1)
    attn_ref[...] = jnp.dot(lhs, mixer_ref[...], preferred_element_type=f32).astype(bf16)
    attn_out = pltpu.make_async_copy(attn_ref, attn_hbm, store_sem.at[0])
    attn_out.start()

    own_back.wait()
    for p in range(1, len(places)):
        returned(p).wait_recv()
    back = back_ref[...].astype(f32).reshape(experts, block, half)
    blank = jnp.zeros((experts, cap, half), f32)
    wide = jnp.concatenate(
        [
            jnp.concatenate([back[:, :cap], blank], axis=1),
            jnp.concatenate([blank, back[:, cap:]], axis=1),
        ],
        axis=2,
    )
    wide = wide.reshape(experts * block, share).astype(bf16)
    moe = jnp.dot(chi_ref[...], wide, preferred_element_type=f32)
    moe = moe + jnp.dot(clo_ref[...], wide, preferred_element_type=f32)
    moe_ref[...] = moe.astype(bf16)
    moe_out = pltpu.make_async_copy(moe_ref, moe_hbm, store_sem.at[1])
    moe_out.start()

    across(0, 1).wait_send()
    for step in range(1, last + 1):
        rightward(step).wait_send()
        if step < last:
            leftward(step).wait_send()
            across(base(step), base(step) + 2).wait_send()
            across(base(step) + 1, base(step) + 3).wait_send()
    across(tail, tail + 1).wait_send()
    for p in range(1, len(places)):
        dispatch(p).wait_send()
        giveback(p).wait_send()
    for which in routed + hidden_units + [attended_all]:
        gone(which)
    attn_out.wait()
    moe_out.wait()


def on_device(
    sizes,
    query_input,
    key_input,
    value_input,
    query_gain,
    key_gain,
    mixer_out,
    moe_input,
    moe_gain,
    routes,
    route_weight,
    expert_gate,
    expert_up,
    expert_down,
):
    Z, Y, X = sizes
    T = Y * X
    experts = Z * CORES
    tokens, columns = query_input.shape
    width = query_gain.shape[0]
    lanes = tokens * (columns // width)
    ep = lax.axis_index("z") * CORES + lax.axis_index("c")
    positions = ep * tokens + jnp.arange(tokens, dtype=jnp.int32)
    cosine, sine = rope_tables(positions, width)
    rows, features = moe_input.shape
    share = features // T
    half = share // 2
    cap = 3 * rows * TOP_K // (2 * experts)
    block = 2 * cap
    hidden = expert_gate.shape[2]
    vmem, anywhere = pltpu.VMEM, pl.BlockSpec(memory_space=pl.ANY)
    bf16, f32 = jnp.bfloat16, jnp.float32
    dma = pltpu.SemaphoreType.DMA
    total = experts * block
    operands = (
        query_input,
        key_input.T,
        value_input.T,
        cosine,
        sine,
        query_gain[None, :],
        key_gain[None, :],
        moe_input,
        moe_gain[None, :],
        routes.T,
        route_weight.T,
        mixer_out,
        expert_gate[0].T,
        expert_up[0].T,
        expert_down[0],
    )
    outs = (
        jax.ShapeDtypeStruct((tokens, mixer_out.shape[1]), bf16),
        jax.ShapeDtypeStruct((rows, share), bf16),
    )
    return pl.pallas_call(
        functools.partial(step_kernel, sizes, cap),
        out_shape=outs,
        in_specs=[anywhere] * len(operands),
        out_specs=(anywhere, anywhere),
        scratch_shapes=[vmem(item.shape, item.dtype) for item in operands + outs]
        + [
            vmem((experts, tokens, 2 * width), bf16),
            vmem((2 * width, lanes), bf16),
            vmem((tokens, lanes), f32),
            vmem((tokens, lanes), f32),
            vmem((8, lanes), f32),
            vmem((8, lanes), f32),
            vmem((8, lanes), f32),
            vmem((16 + width, lanes), f32),
            vmem((experts, rows), f32),
            vmem((experts, rows), f32),
            vmem((total, rows), bf16),
            vmem((total, rows), f32),
            vmem((rows, total), bf16),
            vmem((rows, total), bf16),
            vmem((total, half), bf16),
            vmem((Y, X, total, half), bf16),
            vmem((4 * hidden, T * half), bf16),
            vmem((Y, X, total // 4, 2 * hidden), bf16),
            vmem((total, half), bf16),
            vmem((total, half), bf16),
            vmem((Y, X, tokens, columns), bf16),
            dma((len(operands),)),
            dma((len(outs),)),
        ]
        + [dma((experts,))] * 6
        + [dma((10, 4, 2))] * 2,
        compiler_params=pltpu.CompilerParams(
            collective_id=0, has_side_effects=True, vmem_limit_bytes=60 * 1024 * 1024
        ),
    )(*operands)


def solution(mesh, grid=None):
    n_ep, n_tp = mesh.shape["ep"], mesh.shape["tp"]
    sizes = grid or (n_ep // CORES, 4, n_tp // 4)
    Z, Y, X = sizes
    torus = Mesh(mesh.devices.reshape(Z, CORES, Y, X), AXES)
    ep, tp = ("z", "c"), ("y", "x")
    placed = (
        P(ep, tp),
        P(ep, tp),
        P(ep, tp),
        P(),
        P(),
        P(None, tp),
        P(ep, None),
        P(),
        P(ep, None),
        P(ep, None),
        P(ep, None, tp),
        P(ep, None, tp),
        P(ep, None, tp),
    )
    return jax.shard_map(
        functools.partial(on_device, sizes),
        mesh=torus,
        in_specs=placed,
        out_specs=(P(ep, tp), P(ep, tp)),
        check_vma=False,
    )
```

```python
import functools

import jax
import jax.numpy as jnp
from jax import lax
from jax.experimental import pallas as pl
from jax.experimental.pallas import tpu as pltpu
from jax.sharding import Mesh
from jax.sharding import PartitionSpec as P

GRID_W = 64
TOP_K = 2
CORES = 2
AXES = ("z", "c", "y", "x")
epsilon = 1e-06
base_theta = 10000.0
log2e = 1.4426950408889634
MESH = pl.DeviceIdType.MESH


def rope_tables(positions, head_width):
    quarter = head_width // 4
    inverse = base_theta ** (-jnp.arange(quarter, dtype=jnp.float32) / quarter)
    grid_row = (positions // GRID_W).astype(jnp.float32)
    grid_col = (positions % GRID_W).astype(jnp.float32)
    angles = jnp.concatenate(
        [inverse[:, None] * grid_row[None, :], inverse[:, None] * grid_col[None, :]], axis=0
    )
    return (jnp.cos(angles), jnp.sin(angles))


def rotated(x, cosine, sine, gain):
    scale = lax.rsqrt(jnp.mean(x * x, axis=0, keepdims=True) + epsilon)
    x = x * scale * gain
    half = x.shape[0] // 2
    first, second = x[:half], x[half:]
    return jnp.concatenate(
        [first * cosine - second * sine, first * sine + second * cosine], axis=0
    )


def ring_offsets(size):
    offsets = [0]
    for step in range(1, size // 2 + 1):
        offsets.append(step)
        if step < size - step:
            offsets.append(-step)
    return offsets


def step_kernel(
    sizes,
    cap,
    q_hbm,
    k_hbm,
    v_hbm,
    cos_hbm,
    sin_hbm,
    qg_hbm,
    kg_hbm,
    x_hbm,
    xg_hbm,
    routes_hbm,
    share_hbm,
    mixer_hbm,
    gate_hbm,
    up_hbm,
    down_hbm,
    attn_hbm,
    moe_hbm,
    q_ref,
    k_ref,
    v_ref,
    cos_ref,
    sin_ref,
    qg_ref,
    kg_ref,
    x_ref,
    xg_ref,
    routes_ref,
    share_ref,
    mixer_ref,
    gate_ref,
    up_ref,
    down_ref,
    attn_ref,
    moe_ref,
    kv_ref,
    qt_ref,
    s0_ref,
    s1_ref,
    x0_ref,
    x1_ref,
    m_ref,
    o_ref,
    count_ref,
    weight_ref,
    pick_ref,
    combine_ref,
    chi_ref,
    clo_ref,
    disp_ref,
    rows_ref,
    gu_ref,
    hid_ref,
    eo_ref,
    back_ref,
    att_ref,
    load_sem,
    store_sem,
    kv_send,
    kv_recv,
    d_send,
    d_recv,
    r_send,
    r_recv,
    g_send,
    g_recv,
):
    Z, Y, X = sizes
    T = Y * X
    experts = Z * CORES
    z, c = lax.axis_index("z"), lax.axis_index("c")
    y, x = lax.axis_index("y"), lax.axis_index("x")
    ep = z * CORES + c
    tp = y * X + x
    offsets = ring_offsets(Z)
    places = [(rel, dc) for rel in offsets for dc in range(CORES)]
    block = 2 * cap
    f32, bf16 = jnp.float32, jnp.bfloat16

    def line(rel, dc):
        return {"z": lax.rem(z + (rel + Z), Z), "c": lax.rem(c + dc, CORES)}

    barrier = pltpu.get_barrier_semaphore()
    greeted = 0
    for rel, dc in reversed(places[1:]):
        pl.semaphore_signal(barrier, inc=1, device_id=line(rel, dc), device_id_type=MESH)
        greeted += 1
    for axis, at, size in (("x", x, X), ("y", y, Y)):
        for step in (1, size - 1):
            device = {axis: lax.rem(at + step, size)}
            pl.semaphore_signal(barrier, inc=1, device_id=device, device_id_type=MESH)
            greeted += 1

    pairs = (
        (x_hbm, x_ref),
        (routes_hbm, routes_ref),
        (share_hbm, share_ref),
        (xg_hbm, xg_ref),
        (k_hbm, k_ref),
        (v_hbm, v_ref),
        (cos_hbm, cos_ref),
        (sin_hbm, sin_ref),
        (kg_hbm, kg_ref),
        (q_hbm, q_ref),
        (qg_hbm, qg_ref),
        (gate_hbm, gate_ref),
        (up_hbm, up_ref),
        (down_hbm, down_ref),
        (mixer_hbm, mixer_ref),
    )
    loads = [
        pltpu.make_async_copy(src, dst, load_sem.at[n]) for n, (src, dst) in enumerate(pairs)
    ]
    for load in loads:
        load.start()

    def remote(src, dst, send, recv, device):
        return pltpu.make_async_remote_copy(
            src_ref=src, dst_ref=dst, send_sem=send, recv_sem=recv, device_id=device, device_id_type=MESH
        )

    def column(row):
        return jnp.broadcast_to(row, (8, row.shape[1])).T[:, :1]

    rows, features = x_ref.shape
    share = features // T
    half = share // 2
    for load in loads[1:3]:
        load.wait()
    expert_at = lax.broadcasted_iota(jnp.int32, (experts, rows), 0)
    first = routes_ref[0:1, :] == expert_at
    second = routes_ref[1:2, :] == expert_at
    total_share = share_ref[0:1, :] + share_ref[1:2, :]
    named = jnp.where(first | second, 1.0, 0.0)
    earlier = jnp.where(
        lax.broadcasted_iota(jnp.int32, (rows, rows), 0)
        < lax.broadcasted_iota(jnp.int32, (rows, rows), 1),
        1.0,
        0.0,
    ).astype(bf16)
    count = jnp.dot(named.astype(bf16), earlier, preferred_element_type=f32)
    count_ref[...] = jnp.where(named > 0.0, count, -1.0)
    weight_ref[...] = jnp.where(first, share_ref[0:1, :] / total_share, 0.0) + jnp.where(
        second, share_ref[1:2, :] / total_share, 0.0
    )
    slot_at = lax.broadcasted_iota(jnp.int32, (block, rows), 0)
    slot_at = jnp.where(slot_at < cap, slot_at, slot_at - cap).astype(f32)

    @pl.loop(0, experts)
    def _(expert):
        here = count_ref[pl.ds(expert, 1), :] == slot_at
        at = pl.ds(pl.multiple_of(expert * block, block), block)
        pick_ref[at, :] = jnp.where(here, 1.0, 0.0).astype(bf16)
        combine_ref[at, :] = jnp.where(here, weight_ref[pl.ds(expert, 1), :], 0.0)

    loads[0].wait()
    loads[3].wait()
    chunk = 512
    squares = jnp.zeros((rows, 128), f32)
    for start in range(0, features, chunk):
        part = x_ref[:, start : start + chunk].astype(f32)
        part = part * part
        for lane in range(0, chunk, 128):
            squares = squares + part[:, lane : lane + 128]
    mean = jnp.sum(squares, axis=1, keepdims=True) * (1.0 / features)
    own = pl.ds(pl.multiple_of(tp * share, share), share)
    normed = (x_ref[:, own].astype(f32) * lax.rsqrt(mean + epsilon) * xg_ref[:, own]).astype(bf16)
    picked = jnp.dot(pick_ref[...], normed, preferred_element_type=f32)
    picked = picked.reshape(experts, block, share)
    picked = jnp.concatenate([picked[:, :cap, :half], picked[:, cap:, half:]], axis=1)
    disp_ref[...] = picked.reshape(experts * block, half).astype(bf16)

    for load in loads[4:]:
        load.wait()
    width = k_ref.shape[0]
    k_t = rotated(k_ref[...].astype(f32), cos_ref[...], sin_ref[...], column(kg_ref[...]))
    kv_ref[0] = jnp.concatenate([k_t, v_ref[...].astype(f32)], axis=0).T.astype(bf16)

    tokens = q_ref.shape[0]
    heads = q_ref.shape[1] // width
    lanes = heads * tokens
    q_t = q_ref[...].astype(f32).T
    q_gain = column(qg_ref[...])
    for head in range(heads):
        turned = rotated(
            q_t[head * width : (head + 1) * width], cos_ref[...], sin_ref[...], q_gain
        )
        turned = turned.astype(bf16).astype(f32) * (width ** (-0.5))
        qt_ref[:width, head * tokens : (head + 1) * tokens] = turned.astype(bf16)
    qt_ref[width:, :] = jnp.zeros((width, lanes), bf16)
    m_ref[...] = jnp.full(m_ref.shape, -1e30, f32)
    o_ref[...] = jnp.zeros(o_ref.shape, f32)

    hidden_width = gate_ref.shape[0]
    for t in range(T):
        top, low, to = t * share, t * share + half, t * half
        gu_ref[:, to : to + half] = jnp.concatenate(
            [
                gate_ref[:, top : top + half],
                up_ref[:, top : top + half],
                gate_ref[:, low : low + half],
                up_ref[:, low : low + half],
            ],
            axis=0,
        )
    for e in range(0, experts * block, 256):
        turned = combine_ref[e : e + 256, :].T
        high = turned.astype(bf16)
        chi_ref[:, e : e + 256] = high
        clo_ref[:, e : e + 256] = (turned - high.astype(f32)).astype(bf16)

    pl.semaphore_wait(barrier, greeted)

    def expert_rows(rel, dc):
        target = line(rel, dc)
        return pl.ds(pl.multiple_of((target["z"] * CORES + target["c"]) * block, block), block)

    def dispatch(p):
        rel, dc = places[p]
        return remote(
            disp_ref.at[expert_rows(-rel, dc)],
            rows_ref.at[y, x, pl.ds(p * block, block)],
            d_send.at[p],
            d_recv.at[p],
            line(-rel, dc),
        )

    kept = pltpu.make_async_copy(
        disp_ref.at[expert_rows(0, 0)], rows_ref.at[y, x, pl.ds(0, block)], d_recv.at[0]
    )
    kept.start()
    near = len(places) // 2
    for p in reversed(range(1, near)):
        dispatch(p).start()

    def base(step):
        return 2 + 4 * (step - 1)

    last = Z // 2
    tail = base(last)

    def before(step):
        if isinstance(step, int):
            return 0 if step == 1 else base(step - 1)
        return lax.select(step == 1, 0, base(step - 1))

    def before_left(step):
        if isinstance(step, int):
            return 0 if step == 1 else base(step - 1) + 1
        return lax.select(step == 1, 0, base(step - 1) + 1)

    part_rows = kv_ref.shape[1] // 2

    def moved(src, to, part, device):
        at = pl.ds(part * part_rows, part_rows)
        return remote(
            kv_ref.at[src, at], kv_ref.at[to, at], kv_send.at[to, part], kv_recv.at[to, part], device
        )

    def rightward(step, part):
        return moved(before(step), base(step), part, line(1, 0))

    def leftward(step, part):
        return moved(before_left(step), base(step) + 1, part, line(-1, 0))

    def across(src, to, part):
        return moved(src, to, part, line(0, 1))

    for part in range(2):
        rightward(1, part).start()
        leftward(1, part).start()
        across(0, 1, part).start()
    for p in reversed(range(near, len(places))):
        dispatch(p).start()
    s_ref, mx_ref = (s0_ref, s1_ref), (x0_ref, x1_ref)

    def scores(slot, buffer):
        s = jnp.dot(kv_ref[slot], qt_ref[...], preferred_element_type=f32)
        s_ref[buffer][...] = s
        mx_ref[buffer][...] = jnp.max(s.reshape(tokens // 8, 8, lanes), axis=0)

    def absorb(slot, buffer):
        old = m_ref[...]
        new = jnp.maximum(old, jnp.max(mx_ref[buffer][...], axis=0, keepdims=True) * log2e)
        m_ref[...] = new
        factor = jnp.exp2(old - new)
        p = jnp.exp2(s_ref[buffer][...] * log2e - new[:1]).astype(bf16)
        v_t = kv_ref[slot].T[width:]
        lhs = jnp.concatenate([jnp.ones((16, tokens), bf16), v_t], axis=0)
        part = jnp.dot(lhs, p, preferred_element_type=f32)
        o_ref[...] = o_ref[...] * factor[:1] + part

    def piece_copies(which, kind, j=0):
        ref, pieces, n = which
        found = []
        for number, (begin, length) in enumerate(pieces):
            x_first = number % 2 == 0
            along_x = x_first == (kind in ("near", "far"))
            at, size = (x, X) if along_x else (y, Y)
            other = (x, X) if x_first else (y, Y)
            fixed = lax.rem(other[0] + (0, 3, 2, 1)[j], other[1])
            for way, step in enumerate((1, -1)):
                behind = lax.rem(at - step + size, size)
                device = {"x" if along_x else "y": lax.rem(at + step + size, size)}
                if kind in ("near", "then"):
                    rows_at = pl.ds(begin, length)
                    out_at, in_at = at, behind
                else:
                    rows_at = pl.ds(begin + way * (length // 2), length // 2)
                    out_at, in_at = behind, lax.rem(at + 2, size)

                def view(index):
                    if kind in ("near", "far"):
                        where = (y, index) if along_x else (index, x)
                    else:
                        where = (fixed, index) if along_x else (index, fixed)
                    return ref.at[where[0], where[1], rows_at]

                sem = {"near": 0, "far": 2, "then": 4 + 2 * j, "last": 12 + 2 * j}[kind] + way
                found.append(
                    (view(out_at), view(in_at), g_send.at[n + number, sem], g_recv.at[n + number, sem], device)
                )
        return found

    def go(which, kind, j=0):
        for out, _, send, recv, device in piece_copies(which, kind, j):
            remote(out, out, send, recv, device).start()

    def come(which, kind, j=0):
        for _, into, send, recv, device in piece_copies(which, kind, j):
            remote(into, into, send, recv, device).wait_recv()

    def gone(which):
        kinds = [("near", 0), ("far", 0)] + [(k, j) for k in ("then", "last") for j in range(4)]
        for kind, j in kinds:
            for out, _, send, recv, device in piece_copies(which, kind, j):
                remote(out, out, send, recv, device).wait_send()

    def gather_step(which, number):
        if number == 0:
            go(which, "near")
            go(which, "then", 0)
        elif number == 1:
            come(which, "near")
            go(which, "far")
            go(which, "then", 1)
            go(which, "then", 3)
        elif number == 2:
            come(which, "then", 0)
            go(which, "last", 0)
        elif number == 3:
            come(which, "far")
            go(which, "then", 2)
        elif number == 4:
            come(which, "then", 1)
            come(which, "then", 3)
            go(which, "last", 1)
            go(which, "last", 3)
        elif number == 5:
            come(which, "then", 2)
            go(which, "last", 2)
        else:
            for j in range(4):
                come(which, "last", j)

    groups = 4
    per_group = len(places) // groups
    span = per_group * block
    pack = per_group * cap // 2
    att_half = tokens // 2
    routed = [
        (rows_ref, [(g * span, span) for g in (2 * m, 2 * m + 1)], 2 * m) for m in range(2)
    ]
    hidden_units = [
        (hid_ref, [(g * pack, pack) for g in (2 * m, 2 * m + 1)], 6 + 2 * m) for m in range(2)
    ]
    attended_all = (att_ref, [(0, att_half), (att_half, att_half)], 4)

    def dispatched(m):
        for p in range(2 * m * per_group, 2 * (m + 1) * per_group):
            if p == 0:
                kept.wait()
            else:
                dispatch(p).wait_recv()
        gather_step(routed[m], 0)

    def gate_up(m):
        for group in (2 * m, 2 * m + 1):
            at = pl.ds(group * span, span)
            total = None
            for t in range(0, T, min(T, 4)):
                many = range(t, min(t + 4, T))
                lhs = jnp.concatenate([rows_ref[u // X, u % X, at, :] for u in many], axis=1)
                term = lax.dot_general(
                    lhs,
                    gu_ref[:, t * half : (t + len(many)) * half],
                    (((1,), (1,)), ((), ())),
                    preferred_element_type=f32,
                )
                total = term if total is None else total + term
            both = total.reshape(per_group, block, 4 * hidden_width)
            both = both[:, :cap, : 2 * hidden_width] + both[:, cap:, 2 * hidden_width :]
            both = both.reshape(per_group * cap, 2 * hidden_width)
            gate = both[:, :hidden_width]
            up = both[:, hidden_width:]
            hidden = gate / (1.0 + jnp.exp(-gate)) * up
            hidden = jnp.concatenate([hidden[:pack], hidden[pack:]], axis=1)
            hid_ref[y, x, group * pack : (group + 1) * pack, :] = hidden.astype(bf16)

    def giveback(p):
        rel, dc = places[p]
        mine = pl.ds(pl.multiple_of(ep * block, block), block)
        return remote(
            eo_ref.at[pl.ds(p * block, block)], back_ref.at[mine], r_send.at[p], r_recv.at[p], line(rel, dc)
        )

    def returned(p):
        rel, dc = places[p]
        at = expert_rows(-rel, dc)
        return remote(back_ref.at[at], back_ref.at[at], r_send.at[p], r_recv.at[p], line(rel, dc))

    own_back = pltpu.make_async_copy(
        eo_ref.at[pl.ds(0, block)],
        back_ref.at[pl.ds(pl.multiple_of(ep * block, block), block)],
        r_recv.at[0],
    )

    def down(m):
        gather_step(hidden_units[m], 6)
        for group in (2 * m + 1, 2 * m):
            at = slice(group * pack, (group + 1) * pack)
            lo = jnp.concatenate(
                [hid_ref[u // X, u % X, at, :hidden_width] for u in range(T)], axis=1
            )
            hi = jnp.concatenate(
                [hid_ref[u // X, u % X, at, hidden_width:] for u in range(T)], axis=1
            )
            out = jnp.dot(
                jnp.concatenate([lo, hi], axis=0), down_ref[...], preferred_element_type=f32
            )
            out = out.reshape(per_group, cap, share)
            out = jnp.concatenate([out[:, :, :half], out[:, :, half:]], axis=1)
            eo_ref[group * span : (group + 1) * span, :] = out.reshape(span, half).astype(bf16)
            for p in reversed(range(group * per_group, (group + 1) * per_group)):
                if p == 0:
                    own_back.start()
                else:
                    giveback(p).start()

    def attended_out():
        attended = o_ref[16:, :] / o_ref[:1, :]
        for head in range(heads):
            piece = attended[:, head * tokens : (head + 1) * tokens].T
            att_ref[y, x, :, head * width : (head + 1) * width] = piece.astype(bf16)
        gather_step(attended_all, 0)

    scores(0, 0)
    for part in range(2):
        across(0, 1, part).wait_recv()
    scores(1, 1)
    absorb(0, 0)

    def gather_event(which, number):
        return lambda: gather_step(which, number)

    def last_gate_up(m):
        gather_step(routed[m], 6)
        gate_up(m)
        gather_step(hidden_units[m], 0)

    def at_hidden(m, number):
        return (f"H{m}{number}", gather_event(hidden_units[m], number))

    def at_routed(m, number):
        return (f"G{m}{number}", gather_event(routed[m], number))

    def at_attended(number):
        return (f"A{number}", gather_event(attended_all, number))

    events = {
        (0, 1): [("D0", lambda: dispatched(0))],
        (1, 1): [at_routed(0, n) for n in range(1, 5)],
        (2, 0): [at_routed(0, 5), ("D1", lambda: dispatched(1))],
        (3, 1): [("GU0", lambda: last_gate_up(0))],
        (4, 0): [at_routed(1, 1)],
        (4, 1): [at_hidden(0, 1), at_routed(1, 2)],
        (5, 0): [at_routed(1, 3), at_hidden(0, 2)],
        (5, 1): [at_hidden(0, 3)],
        (6, 0): [at_routed(1, 4), at_hidden(0, 4)],
        (6, 1): [at_routed(1, 5), at_hidden(0, 5)],
        (7, 1): [("GU1", lambda: last_gate_up(1)), ("DN0", lambda: down(0))],
        (8, 0): [at_hidden(1, 1)],
        (8, 1): [at_hidden(1, 2), at_hidden(1, 3)],
        (9, 1): [
            at_hidden(1, 5),
            ("ATT", attended_out),
            ("DN1", lambda: down(1)),
        ]
        + [at_attended(n) for n in range(1, 7)],
        (8, 2): [at_hidden(1, 4)],
    }

    def run(number):
        for name, event in events.get(number, ()):
            event()

    run((0, 1))

    @pl.loop(1, last)
    def _(step):
        at = base(step)
        for part in range(2):
            rightward(step, part).wait_recv()
            rightward(step + 1, part).start()
            across(at, at + 2, part).start()
            leftward(step, part).wait_recv()

            @pl.when(step < last - 1)
            def _(part=part):
                leftward(step + 1, part).start()

            across(at + 1, at + 3, part).start()
            for number in range(1, last):
                if (number, part) in events:

                    @pl.when(step == number)
                    def _(number=number, part=part):
                        run((number, part))

            @pl.when(step > 1)
            def _(part=part):
                even = at - 4 + 2 * part
                if part == 1:
                    for other in range(2):
                        across(at - 4, at - 2, other).wait_recv()
                        across(at - 3, at - 1, other).wait_recv()
                scores(even, 0)
                absorb(even - 1, 1)
                scores(even + 1, 1)
                absorb(even, 0)

    for part in range(2):
        rightward(last, part).wait_recv()
        across(tail, tail + 1, part).start()
    run((8, 0))

    @pl.loop(0, 2)
    def _(pair):
        even = tail - 4 + 2 * pair

        @pl.when(pair == 1)
        def _():
            for part in range(2):
                across(tail - 4, tail - 2, part).wait_recv()
                across(tail - 3, tail - 1, part).wait_recv()

        scores(even, 0)
        absorb(even - 1, 1)
        scores(even + 1, 1)
        absorb(even, 0)

    run((8, 1))
    scores(tail, 0)
    absorb(tail - 1, 1)
    run((8, 2))
    for part in range(2):
        across(tail, tail + 1, part).wait_recv()
    scores(tail + 1, 1)
    absorb(tail, 0)
    absorb(tail + 1, 1)
    run((9, 1))

    lhs = jnp.concatenate([att_ref[u // X, u % X] for u in range(T)], axis=1)
    attn_ref[...] = jnp.dot(lhs, mixer_ref[...], preferred_element_type=f32).astype(bf16)
    attn_out = pltpu.make_async_copy(attn_ref, attn_hbm, store_sem.at[0])
    attn_out.start()

    own_back.wait()
    for p in range(1, len(places)):
        returned(p).wait_recv()
    back = back_ref[...].astype(f32).reshape(experts, block, half)
    blank = jnp.zeros((experts, cap, half), f32)
    wide = jnp.concatenate(
        [
            jnp.concatenate([back[:, :cap], blank], axis=1),
            jnp.concatenate([blank, back[:, cap:]], axis=1),
        ],
        axis=2,
    )
    wide = wide.reshape(experts * block, share).astype(bf16)
    moe = jnp.dot(chi_ref[...], wide, preferred_element_type=f32)
    moe = moe + jnp.dot(clo_ref[...], wide, preferred_element_type=f32)
    moe_ref[...] = moe.astype(bf16)
    moe_out = pltpu.make_async_copy(moe_ref, moe_hbm, store_sem.at[1])
    moe_out.start()

    for part in range(2):
        across(0, 1, part).wait_send()
        for step in range(1, last + 1):
            rightward(step, part).wait_send()
            if step < last:
                leftward(step, part).wait_send()
                across(base(step), base(step) + 2, part).wait_send()
                across(base(step) + 1, base(step) + 3, part).wait_send()
        across(tail, tail + 1, part).wait_send()
    for p in range(1, len(places)):
        dispatch(p).wait_send()
        giveback(p).wait_send()
    for which in routed + hidden_units + [attended_all]:
        gone(which)
    attn_out.wait()
    moe_out.wait()


def hand_over_kernel(a_in, b_in, a_out, b_out, a_ref, b_ref, sem):
    moves = [
        (pltpu.make_async_copy(src, ref, sem.at[n]), pltpu.make_async_copy(ref, dst, sem.at[n + 2]))
        for n, (src, ref, dst) in enumerate(((a_in, a_ref, a_out), (b_in, b_ref, b_out)))
    ]
    for into, _ in moves:
        into.start()
    for into, out in moves:
        into.wait()
        out.start()
    for _, out in moves:
        out.wait()


def on_device(
    sizes,
    query_input,
    key_input,
    value_input,
    query_gain,
    key_gain,
    mixer_out,
    moe_input,
    moe_gain,
    routes,
    route_weight,
    expert_gate,
    expert_up,
    expert_down,
):
    Z, Y, X = sizes
    T = Y * X
    experts = Z * CORES
    tokens, columns = query_input.shape
    width = query_gain.shape[0]
    lanes = tokens * (columns // width)
    ep = lax.axis_index("z") * CORES + lax.axis_index("c")
    positions = ep * tokens + jnp.arange(tokens, dtype=jnp.int32)
    cosine, sine = rope_tables(positions, width)
    rows, features = moe_input.shape
    share = features // T
    half = share // 2
    cap = 3 * rows * TOP_K // (2 * experts)
    block = 2 * cap
    hidden = expert_gate.shape[2]
    vmem, anywhere = pltpu.VMEM, pl.BlockSpec(memory_space=pl.ANY)
    bf16, f32 = jnp.bfloat16, jnp.float32
    dma = pltpu.SemaphoreType.DMA
    total = experts * block
    operands = (
        query_input,
        key_input.T,
        value_input.T,
        cosine,
        sine,
        query_gain[None, :],
        key_gain[None, :],
        moe_input,
        moe_gain[None, :],
        routes.T,
        route_weight.T,
        mixer_out,
        expert_gate[0].T,
        expert_up[0].T,
        expert_down[0],
    )
    outs = (
        jax.ShapeDtypeStruct((tokens, mixer_out.shape[1]), bf16),
        jax.ShapeDtypeStruct((rows, share), bf16),
    )
    results = pl.pallas_call(
        functools.partial(step_kernel, sizes, cap),
        out_shape=outs,
        in_specs=[anywhere] * len(operands),
        out_specs=(anywhere, anywhere),
        scratch_shapes=[vmem(item.shape, item.dtype) for item in operands + outs]
        + [
            vmem((experts, tokens, 2 * width), bf16),
            vmem((2 * width, lanes), bf16),
            vmem((tokens, lanes), f32),
            vmem((tokens, lanes), f32),
            vmem((8, lanes), f32),
            vmem((8, lanes), f32),
            vmem((8, lanes), f32),
            vmem((16 + width, lanes), f32),
            vmem((experts, rows), f32),
            vmem((experts, rows), f32),
            vmem((total, rows), bf16),
            vmem((total, rows), f32),
            vmem((rows, total), bf16),
            vmem((rows, total), bf16),
            vmem((total, half), bf16),
            vmem((Y, X, total, half), bf16),
            vmem((4 * hidden, T * half), bf16),
            vmem((Y, X, total // 4, 2 * hidden), bf16),
            vmem((total, half), bf16),
            vmem((total, half), bf16),
            vmem((Y, X, tokens, columns), bf16),
            dma((len(operands),)),
            dma((len(outs),)),
        ]
        + [dma((experts, 2))] * 2
        + [dma((experts,))] * 4
        + [dma((10, 20))] * 2,
        compiler_params=pltpu.CompilerParams(
            collective_id=0, has_side_effects=True, vmem_limit_bytes=60 * 1024 * 1024
        ),
    )(*operands)
    return pl.pallas_call(
        hand_over_kernel,
        out_shape=outs,
        in_specs=[anywhere] * 2,
        out_specs=(anywhere, anywhere),
        scratch_shapes=[vmem(item.shape, item.dtype) for item in outs] + [dma((4,))],
    )(*results)


def solution(mesh, grid=None):
    n_ep, n_tp = mesh.shape["ep"], mesh.shape["tp"]
    sizes = grid or (n_ep // CORES, 4, n_tp // 4)
    Z, Y, X = sizes
    torus = Mesh(mesh.devices.reshape(Z, CORES, Y, X), AXES)
    ep, tp = ("z", "c"), ("y", "x")
    placed = (
        P(ep, tp),
        P(ep, tp),
        P(ep, tp),
        P(),
        P(),
        P(None, tp),
        P(ep, None),
        P(),
        P(ep, None),
        P(ep, None),
        P(ep, None, tp),
        P(ep, None, tp),
        P(ep, None, tp),
    )
    return jax.shard_map(
        functools.partial(on_device, sizes),
        mesh=torus,
        in_specs=placed,
        out_specs=(P(ep, tp), P(ep, tp)),
        check_vma=False,
    )
```

```python
import functools

import jax
import jax.numpy as jnp
from jax import lax
from jax.experimental import pallas as pl
from jax.experimental.pallas import tpu as pltpu
from jax.sharding import Mesh
from jax.sharding import PartitionSpec as P

GRID_W = 64
TOP_K = 2
CORES = 2
AXES = ("z", "c", "y", "x")
epsilon = 1e-06
base_theta = 10000.0
log2e = 1.4426950408889634
MESH = pl.DeviceIdType.MESH


def rope_tables(positions, head_width):
    quarter = head_width // 4
    inverse = base_theta ** (-jnp.arange(quarter, dtype=jnp.float32) / quarter)
    grid_row = (positions // GRID_W).astype(jnp.float32)
    grid_col = (positions % GRID_W).astype(jnp.float32)
    angles = jnp.concatenate(
        [inverse[:, None] * grid_row[None, :], inverse[:, None] * grid_col[None, :]], axis=0
    )
    return (jnp.cos(angles), jnp.sin(angles))


def rotated(x, cosine, sine, gain):
    scale = lax.rsqrt(jnp.mean(x * x, axis=0, keepdims=True) + epsilon)
    x = x * scale * gain
    half = x.shape[0] // 2
    first, second = x[:half], x[half:]
    return jnp.concatenate(
        [first * cosine - second * sine, first * sine + second * cosine], axis=0
    )


def ring_offsets(size):
    offsets = [0]
    for step in range(1, size // 2 + 1):
        offsets.append(step)
        if step < size - step:
            offsets.append(-step)
    return offsets


def step_kernel(
    sizes,
    cap,
    q_hbm,
    k_hbm,
    v_hbm,
    cos_hbm,
    sin_hbm,
    qg_hbm,
    kg_hbm,
    x_hbm,
    xg_hbm,
    routes_hbm,
    share_hbm,
    mixer_hbm,
    gate_hbm,
    up_hbm,
    down_hbm,
    attn_hbm,
    moe_hbm,
    q_ref,
    k_ref,
    v_ref,
    cos_ref,
    sin_ref,
    qg_ref,
    kg_ref,
    x_ref,
    xg_ref,
    routes_ref,
    share_ref,
    mixer_ref,
    gate_ref,
    up_ref,
    down_ref,
    attn_ref,
    moe_ref,
    kv_ref,
    qt_ref,
    s0_ref,
    s1_ref,
    x0_ref,
    x1_ref,
    m_ref,
    o_ref,
    count_ref,
    weight_ref,
    pick_ref,
    combine_ref,
    chi_ref,
    clo_ref,
    disp_ref,
    rows_ref,
    gu_ref,
    hid_ref,
    eo_ref,
    back_ref,
    att_ref,
    load_sem,
    store_sem,
    kv_send,
    kv_recv,
    d_send,
    d_recv,
    r_send,
    r_recv,
    g_send,
    g_recv,
    own_sem,
):
    Z, Y, X = sizes
    T = Y * X
    experts = Z * CORES
    z, c = lax.axis_index("z"), lax.axis_index("c")
    y, x = lax.axis_index("y"), lax.axis_index("x")
    ep = z * CORES + c
    tp = y * X + x
    offsets = ring_offsets(Z)
    places = [(rel, dc) for rel in offsets for dc in range(CORES)]
    block = 2 * cap
    f32, bf16 = jnp.float32, jnp.bfloat16

    def line(rel, dc):
        return {"z": lax.rem(z + (rel + Z), Z), "c": lax.rem(c + dc, CORES)}

    barrier = pltpu.get_barrier_semaphore()
    greeted = 0
    for rel, dc in reversed(places[1:]):
        pl.semaphore_signal(barrier, inc=1, device_id=line(rel, dc), device_id_type=MESH)
        greeted += 1
    for axis, at, size in (("x", x, X), ("y", y, Y)):
        for step in (1, size - 1):
            device = {axis: lax.rem(at + step, size)}
            pl.semaphore_signal(barrier, inc=1, device_id=device, device_id_type=MESH)
            greeted += 1

    pairs = (
        (x_hbm, x_ref),
        (routes_hbm, routes_ref),
        (share_hbm, share_ref),
        (xg_hbm, xg_ref),
        (k_hbm, k_ref),
        (v_hbm, v_ref),
        (cos_hbm, cos_ref),
        (sin_hbm, sin_ref),
        (kg_hbm, kg_ref),
        (q_hbm, q_ref),
        (qg_hbm, qg_ref),
        (gate_hbm, gate_ref),
        (up_hbm, up_ref),
        (down_hbm, down_ref),
        (mixer_hbm, mixer_ref),
    )
    loads = [
        pltpu.make_async_copy(src, dst, load_sem.at[n]) for n, (src, dst) in enumerate(pairs)
    ]
    for load in loads:
        load.start()

    def remote(src, dst, send, recv, device):
        return pltpu.make_async_remote_copy(
            src_ref=src, dst_ref=dst, send_sem=send, recv_sem=recv, device_id=device, device_id_type=MESH
        )

    def column(row):
        return jnp.broadcast_to(row, (8, row.shape[1])).T[:, :1]

    rows, features = x_ref.shape
    share = features // T
    half = share // 2
    for load in loads[1:3]:
        load.wait()
    expert_at = lax.broadcasted_iota(jnp.int32, (experts, rows), 0)
    first = routes_ref[0:1, :] == expert_at
    second = routes_ref[1:2, :] == expert_at
    total_share = share_ref[0:1, :] + share_ref[1:2, :]
    named = jnp.where(first | second, 1.0, 0.0)
    earlier = jnp.where(
        lax.broadcasted_iota(jnp.int32, (rows, rows), 0)
        < lax.broadcasted_iota(jnp.int32, (rows, rows), 1),
        1.0,
        0.0,
    ).astype(bf16)
    count = jnp.dot(named.astype(bf16), earlier, preferred_element_type=f32)
    count_ref[...] = jnp.where(named > 0.0, count, -1.0)
    weight_ref[...] = jnp.where(first, share_ref[0:1, :] / total_share, 0.0) + jnp.where(
        second, share_ref[1:2, :] / total_share, 0.0
    )
    slot_at = lax.broadcasted_iota(jnp.int32, (block, rows), 0)
    slot_at = jnp.where(slot_at < cap, slot_at, slot_at - cap).astype(f32)

    @pl.loop(0, experts)
    def _(expert):
        here = count_ref[pl.ds(expert, 1), :] == slot_at
        at = pl.ds(pl.multiple_of(expert * block, block), block)
        pick_ref[at, :] = jnp.where(here, 1.0, 0.0).astype(bf16)
        combine_ref[at, :] = jnp.where(here, weight_ref[pl.ds(expert, 1), :], 0.0)

    loads[0].wait()
    loads[3].wait()
    chunk = 512
    squares = jnp.zeros((rows, 128), f32)
    for start in range(0, features, chunk):
        part = x_ref[:, start : start + chunk].astype(f32)
        part = part * part
        for lane in range(0, chunk, 128):
            squares = squares + part[:, lane : lane + 128]
    mean = jnp.sum(squares, axis=1, keepdims=True) * (1.0 / features)
    own = pl.ds(pl.multiple_of(tp * share, share), share)
    normed = (x_ref[:, own].astype(f32) * lax.rsqrt(mean + epsilon) * xg_ref[:, own]).astype(bf16)
    picked = jnp.dot(pick_ref[...], normed, preferred_element_type=f32)
    picked = picked.reshape(experts, block, share)
    picked = jnp.concatenate([picked[:, :cap, :half], picked[:, cap:, half:]], axis=1)
    disp_ref[...] = picked.reshape(experts * block, half).astype(bf16)

    for load in loads[4:]:
        load.wait()
    width = k_ref.shape[0]
    k_t = rotated(k_ref[...].astype(f32), cos_ref[...], sin_ref[...], column(kg_ref[...]))
    kv_ref[0] = jnp.concatenate([k_t, v_ref[...].astype(f32)], axis=0).T.astype(bf16)

    tokens = q_ref.shape[0]
    heads = q_ref.shape[1] // width
    lanes = heads * tokens
    q_t = q_ref[...].astype(f32).T
    q_gain = column(qg_ref[...])
    for head in range(heads):
        turned = rotated(
            q_t[head * width : (head + 1) * width], cos_ref[...], sin_ref[...], q_gain
        )
        turned = turned.astype(bf16).astype(f32) * (width ** (-0.5))
        qt_ref[:width, head * tokens : (head + 1) * tokens] = turned.astype(bf16)
    qt_ref[width:, :] = jnp.zeros((width, lanes), bf16)
    m_ref[...] = jnp.full(m_ref.shape, -1e30, f32)
    o_ref[...] = jnp.zeros(o_ref.shape, f32)

    hidden_width = gate_ref.shape[0]
    for t in range(T):
        top, low, to = t * share, t * share + half, t * half
        gu_ref[:, to : to + half] = jnp.concatenate(
            [
                gate_ref[:, top : top + half],
                up_ref[:, top : top + half],
                gate_ref[:, low : low + half],
                up_ref[:, low : low + half],
            ],
            axis=0,
        )
    for e in range(0, experts * block, 256):
        turned = combine_ref[e : e + 256, :].T
        high = turned.astype(bf16)
        chi_ref[:, e : e + 256] = high
        clo_ref[:, e : e + 256] = (turned - high.astype(f32)).astype(bf16)

    pl.semaphore_wait(barrier, greeted)

    def expert_rows(rel, dc):
        target = line(rel, dc)
        return pl.ds(pl.multiple_of((target["z"] * CORES + target["c"]) * block, block), block)

    def dispatch(p):
        rel, dc = places[p]
        return remote(
            disp_ref.at[expert_rows(-rel, dc)],
            rows_ref.at[y, x, pl.ds(p * block, block)],
            d_send.at[0],
            d_recv.at[0 if p < len(places) // 2 else 1],
            line(-rel, dc),
        )

    kept = pltpu.make_async_copy(
        disp_ref.at[expert_rows(0, 0)], rows_ref.at[y, x, pl.ds(0, block)], own_sem.at[0]
    )
    kept.start()
    near = len(places) // 2
    for p in reversed(range(1, near)):
        dispatch(p).start()

    def base(step):
        return 2 + 4 * (step - 1)

    last = Z // 2
    tail = base(last)

    def before(step):
        if isinstance(step, int):
            return 0 if step == 1 else base(step - 1)
        return lax.select(step == 1, 0, base(step - 1))

    def before_left(step):
        if isinstance(step, int):
            return 0 if step == 1 else base(step - 1) + 1
        return lax.select(step == 1, 0, base(step - 1) + 1)

    part_rows = kv_ref.shape[1] // 2

    def moved(src, to, part, device):
        at = pl.ds(part * part_rows, part_rows)
        return remote(
            kv_ref.at[src, at], kv_ref.at[to, at], kv_send.at[0], kv_recv.at[to, part], device
        )

    def rightward(step, part):
        return moved(before(step), base(step), part, line(1, 0))

    def leftward(step, part):
        return moved(before_left(step), base(step) + 1, part, line(-1, 0))

    def across(src, to, part):
        return moved(src, to, part, line(0, 1))

    for part in range(2):
        rightward(1, part).start()
        leftward(1, part).start()
        across(0, 1, part).start()
    for p in reversed(range(near, len(places))):
        dispatch(p).start()
    s_ref, mx_ref = (s0_ref, s1_ref), (x0_ref, x1_ref)

    def scores(slot, buffer):
        s = jnp.dot(kv_ref[slot], qt_ref[...], preferred_element_type=f32)
        s_ref[buffer][...] = s
        mx_ref[buffer][...] = jnp.max(s.reshape(tokens // 8, 8, lanes), axis=0)

    def absorb(slot, buffer):
        old = m_ref[...]
        new = jnp.maximum(old, jnp.max(mx_ref[buffer][...], axis=0, keepdims=True) * log2e)
        m_ref[...] = new
        factor = jnp.exp2(old - new)
        p = jnp.exp2(s_ref[buffer][...] * log2e - new[:1]).astype(bf16)
        v_t = kv_ref[slot].T[width:]
        lhs = jnp.concatenate([jnp.ones((16, tokens), bf16), v_t], axis=0)
        part = jnp.dot(lhs, p, preferred_element_type=f32)
        o_ref[...] = o_ref[...] * factor[:1] + part

    def piece_copies(which, kind, j=0):
        ref, pieces, n = which
        found = []
        for number, (begin, length) in enumerate(pieces):
            x_first = number % 2 == 0
            along_x = x_first == (kind in ("near", "far"))
            at, size = (x, X) if along_x else (y, Y)
            other = (x, X) if x_first else (y, Y)
            fixed = lax.rem(other[0] + (0, 3, 2, 1)[j], other[1])
            for way, step in enumerate((1, -1)):
                behind = lax.rem(at - step + size, size)
                device = {"x" if along_x else "y": lax.rem(at + step + size, size)}
                if kind in ("near", "then"):
                    rows_at = pl.ds(begin, length)
                    out_at, in_at = at, behind
                else:
                    rows_at = pl.ds(begin + way * (length // 2), length // 2)
                    out_at, in_at = behind, lax.rem(at + 2, size)

                def view(index):
                    if kind in ("near", "far"):
                        where = (y, index) if along_x else (index, x)
                    else:
                        where = (fixed, index) if along_x else (index, fixed)
                    return ref.at[where[0], where[1], rows_at]

                sem = {"near": 0, "far": 2, "then": 4 + 2 * j, "last": 12 + 2 * j}[kind] + way
                found.append(
                    (view(out_at), view(in_at), g_send.at[(n + number) // 2], g_recv.at[n + number, sem], device)
                )
        return found

    def go(which, kind, j=0):
        for out, _, send, recv, device in piece_copies(which, kind, j):
            remote(out, out, send, recv, device).start()

    def come(which, kind, j=0):
        for _, into, send, recv, device in piece_copies(which, kind, j):
            remote(into, into, send, recv, device).wait_recv()

    def gone(which):
        ref, pieces, n = which
        rows_sent = 15 * len(pieces) * pieces[0][1]
        cells = 12 if rows_sent // 12 <= ref.shape[2] else 16
        view = ref.at[:, pl.ds(0, cells // Y), pl.ds(0, rows_sent // cells)]
        remote(view, view, g_send.at[n // 2], g_recv.at[0, 0], line(0, 1)).wait_send()

    def gather_step(which, number):
        if number == 0:
            go(which, "near")
            go(which, "then", 0)
        elif number == 1:
            come(which, "near")
            go(which, "far")
            go(which, "then", 1)
            go(which, "then", 3)
        elif number == 2:
            come(which, "then", 0)
            go(which, "last", 0)
        elif number == 3:
            come(which, "far")
            go(which, "then", 2)
        elif number == 4:
            come(which, "then", 1)
            come(which, "then", 3)
            go(which, "last", 1)
            go(which, "last", 3)
        elif number == 5:
            come(which, "then", 2)
            go(which, "last", 2)
        else:
            for j in range(4):
                come(which, "last", j)

    groups = 4
    per_group = len(places) // groups
    span = per_group * block
    pack = per_group * cap // 2
    att_half = tokens // 2
    routed = [
        (rows_ref, [(g * span, span) for g in (2 * m, 2 * m + 1)], 2 * m) for m in range(2)
    ]
    hidden_units = [
        (hid_ref, [(g * pack, pack) for g in (2 * m, 2 * m + 1)], 6 + 2 * m) for m in range(2)
    ]
    attended_all = (att_ref, [(0, att_half), (att_half, att_half)], 4)

    def dispatched(m):
        if m == 0:
            kept.wait()
        begin = max(1, m * near) * block
        here = rows_ref.at[y, x, pl.ds(begin, (m + 1) * near * block - begin)]
        remote(here, here, d_send.at[0], d_recv.at[m], line(0, 1)).wait_recv()
        gather_step(routed[m], 0)

    def gate_up(m):
        for group in (2 * m, 2 * m + 1):
            at = pl.ds(group * span, span)
            total = None
            for t in range(0, T, min(T, 4)):
                many = range(t, min(t + 4, T))
                lhs = jnp.concatenate([rows_ref[u // X, u % X, at, :] for u in many], axis=1)
                term = lax.dot_general(
                    lhs,
                    gu_ref[:, t * half : (t + len(many)) * half],
                    (((1,), (1,)), ((), ())),
                    preferred_element_type=f32,
                )
                total = term if total is None else total + term
            both = total.reshape(per_group, block, 4 * hidden_width)
            both = both[:, :cap, : 2 * hidden_width] + both[:, cap:, 2 * hidden_width :]
            both = both.reshape(per_group * cap, 2 * hidden_width)
            gate = both[:, :hidden_width]
            up = both[:, hidden_width:]
            hidden = gate / (1.0 + jnp.exp(-gate)) * up
            hidden = jnp.concatenate([hidden[:pack], hidden[pack:]], axis=1)
            hid_ref[y, x, group * pack : (group + 1) * pack, :] = hidden.astype(bf16)

    def giveback(p):
        rel, dc = places[p]
        mine = pl.ds(pl.multiple_of(ep * block, block), block)
        return remote(
            eo_ref.at[pl.ds(p * block, block)], back_ref.at[mine], r_send.at[0], r_recv.at[0], line(rel, dc)
        )

    own_back = pltpu.make_async_copy(
        eo_ref.at[pl.ds(0, block)],
        back_ref.at[pl.ds(pl.multiple_of(ep * block, block), block)],
        own_sem.at[1],
    )

    def down(m):
        gather_step(hidden_units[m], 6)
        for group in (2 * m + 1, 2 * m):
            at = slice(group * pack, (group + 1) * pack)
            lo = jnp.concatenate(
                [hid_ref[u // X, u % X, at, :hidden_width] for u in range(T)], axis=1
            )
            hi = jnp.concatenate(
                [hid_ref[u // X, u % X, at, hidden_width:] for u in range(T)], axis=1
            )
            out = jnp.dot(
                jnp.concatenate([lo, hi], axis=0), down_ref[...], preferred_element_type=f32
            )
            out = out.reshape(per_group, cap, share)
            out = jnp.concatenate([out[:, :, :half], out[:, :, half:]], axis=1)
            eo_ref[group * span : (group + 1) * span, :] = out.reshape(span, half).astype(bf16)
            for p in reversed(range(group * per_group, (group + 1) * per_group)):
                if p == 0:
                    own_back.start()
                else:
                    giveback(p).start()

    def attended_out():
        attended = o_ref[16:, :] / o_ref[:1, :]
        for head in range(heads):
            piece = attended[:, head * tokens : (head + 1) * tokens].T
            att_ref[y, x, :, head * width : (head + 1) * width] = piece.astype(bf16)
        gather_step(attended_all, 0)

    scores(0, 0)
    for part in range(2):
        across(0, 1, part).wait_recv()
    scores(1, 1)
    absorb(0, 0)

    def gather_event(which, number):
        return lambda: gather_step(which, number)

    def last_gate_up(m):
        gather_step(routed[m], 6)
        gate_up(m)
        gather_step(hidden_units[m], 0)

    def at_hidden(m, number):
        return (f"H{m}{number}", gather_event(hidden_units[m], number))

    def at_routed(m, number):
        return (f"G{m}{number}", gather_event(routed[m], number))

    def at_attended(number):
        return (f"A{number}", gather_event(attended_all, number))

    events = {
        (0, 1): [("D0", lambda: dispatched(0))],
        (1, 1): [at_routed(0, n) for n in range(1, 5)],
        (2, 0): [at_routed(0, 5), ("D1", lambda: dispatched(1))],
        (3, 1): [("GU0", lambda: last_gate_up(0))],
        (4, 0): [at_routed(1, 1)],
        (4, 1): [at_hidden(0, 1), at_routed(1, 2)],
        (5, 0): [at_routed(1, 3), at_hidden(0, 2)],
        (5, 1): [at_hidden(0, 3)],
        (6, 0): [at_routed(1, 4), at_hidden(0, 4)],
        (6, 1): [at_routed(1, 5), at_hidden(0, 5)],
        (7, 1): [("GU1", lambda: last_gate_up(1)), ("DN0", lambda: down(0))],
        (8, 0): [at_hidden(1, 1)],
        (8, 1): [at_hidden(1, 2), at_hidden(1, 3)],
        (9, 1): [
            at_hidden(1, 5),
            ("ATT", attended_out),
            ("DN1", lambda: down(1)),
        ]
        + [at_attended(n) for n in range(1, 7)],
        (8, 2): [at_hidden(1, 4)],
    }

    def run(number):
        for name, event in events.get(number, ()):
            event()

    run((0, 1))

    @pl.loop(1, last)
    def _(step):
        at = base(step)
        for part in range(2):
            rightward(step, part).wait_recv()
            rightward(step + 1, part).start()
            across(at, at + 2, part).start()
            leftward(step, part).wait_recv()

            @pl.when(step < last - 1)
            def _(part=part):
                leftward(step + 1, part).start()

            across(at + 1, at + 3, part).start()
            for number in range(1, last):
                if (number, part) in events:

                    @pl.when(step == number)
                    def _(number=number, part=part):
                        run((number, part))

            @pl.when(step > 1)
            def _(part=part):
                even = at - 4 + 2 * part
                if part == 1:
                    for other in range(2):
                        across(at - 4, at - 2, other).wait_recv()
                        across(at - 3, at - 1, other).wait_recv()
                scores(even, 0)
                absorb(even - 1, 1)
                scores(even + 1, 1)
                absorb(even, 0)

    for part in range(2):
        rightward(last, part).wait_recv()
        across(tail, tail + 1, part).start()
    run((8, 0))

    @pl.loop(0, 2)
    def _(pair):
        even = tail - 4 + 2 * pair

        @pl.when(pair == 1)
        def _():
            for part in range(2):
                across(tail - 4, tail - 2, part).wait_recv()
                across(tail - 3, tail - 1, part).wait_recv()

        scores(even, 0)
        absorb(even - 1, 1)
        scores(even + 1, 1)
        absorb(even, 0)

    run((8, 1))
    scores(tail, 0)
    absorb(tail - 1, 1)
    run((8, 2))
    for part in range(2):
        across(tail, tail + 1, part).wait_recv()
    scores(tail + 1, 1)
    absorb(tail, 0)
    absorb(tail + 1, 1)
    run((9, 1))

    lhs = jnp.concatenate([att_ref[u // X, u % X] for u in range(T)], axis=1)
    attn_ref[...] = jnp.dot(lhs, mixer_ref[...], preferred_element_type=f32).astype(bf16)
    attn_out = pltpu.make_async_copy(attn_ref, attn_hbm, store_sem.at[0])
    attn_out.start()

    own_back.wait()
    others = pl.ds(0, (len(places) - 1) * block)
    remote(
        back_ref.at[others], back_ref.at[others], r_send.at[0], r_recv.at[0], line(0, 1)
    ).wait_recv()
    back = back_ref[...].astype(f32).reshape(experts, block, half)
    blank = jnp.zeros((experts, cap, half), f32)
    wide = jnp.concatenate(
        [
            jnp.concatenate([back[:, :cap], blank], axis=1),
            jnp.concatenate([blank, back[:, cap:]], axis=1),
        ],
        axis=2,
    )
    wide = wide.reshape(experts * block, share).astype(bf16)
    moe = jnp.dot(chi_ref[...], wide, preferred_element_type=f32)
    moe = moe + jnp.dot(clo_ref[...], wide, preferred_element_type=f32)
    moe_ref[...] = moe.astype(bf16)
    moe_out = pltpu.make_async_copy(moe_ref, moe_hbm, store_sem.at[1])
    moe_out.start()

    chunks = pl.ds(0, kv_ref.shape[0] - 1)
    for ref, at, send, recv in (
        (kv_ref, chunks, kv_send.at[0], kv_recv.at[0, 0]),
        (disp_ref, others, d_send.at[0], d_recv.at[0]),
        (eo_ref, others, r_send.at[0], r_recv.at[0]),
    ):
        remote(ref.at[at], ref.at[at], send, recv, line(0, 1)).wait_send()
    for which in routed + hidden_units + [attended_all]:
        gone(which)
    attn_out.wait()
    moe_out.wait()


def hand_over_kernel(a_in, b_in, a_out, b_out, a_ref, b_ref, sem):
    moves = [
        (pltpu.make_async_copy(src, ref, sem.at[n]), pltpu.make_async_copy(ref, dst, sem.at[n + 2]))
        for n, (src, ref, dst) in enumerate(((a_in, a_ref, a_out), (b_in, b_ref, b_out)))
    ]
    for into, _ in moves:
        into.start()
    for into, out in moves:
        into.wait()
        out.start()
    for _, out in moves:
        out.wait()


def on_device(
    sizes,
    query_input,
    key_input,
    value_input,
    query_gain,
    key_gain,
    mixer_out,
    moe_input,
    moe_gain,
    routes,
    route_weight,
    expert_gate,
    expert_up,
    expert_down,
):
    Z, Y, X = sizes
    T = Y * X
    experts = Z * CORES
    tokens, columns = query_input.shape
    width = query_gain.shape[0]
    lanes = tokens * (columns // width)
    ep = lax.axis_index("z") * CORES + lax.axis_index("c")
    positions = ep * tokens + jnp.arange(tokens, dtype=jnp.int32)
    cosine, sine = rope_tables(positions, width)
    rows, features = moe_input.shape
    share = features // T
    half = share // 2
    cap = 3 * rows * TOP_K // (2 * experts)
    block = 2 * cap
    hidden = expert_gate.shape[2]
    vmem, anywhere = pltpu.VMEM, pl.BlockSpec(memory_space=pl.ANY)
    bf16, f32 = jnp.bfloat16, jnp.float32
    dma = pltpu.SemaphoreType.DMA
    total = experts * block
    operands = (
        query_input,
        key_input.T,
        value_input.T,
        cosine,
        sine,
        query_gain[None, :],
        key_gain[None, :],
        moe_input,
        moe_gain[None, :],
        routes.T,
        route_weight.T,
        mixer_out,
        expert_gate[0].T,
        expert_up[0].T,
        expert_down[0],
    )
    outs = (
        jax.ShapeDtypeStruct((tokens, mixer_out.shape[1]), bf16),
        jax.ShapeDtypeStruct((rows, share), bf16),
    )
    results = pl.pallas_call(
        functools.partial(step_kernel, sizes, cap),
        out_shape=outs,
        in_specs=[anywhere] * len(operands),
        out_specs=(anywhere, anywhere),
        scratch_shapes=[vmem(item.shape, item.dtype) for item in operands + outs]
        + [
            vmem((experts, tokens, 2 * width), bf16),
            vmem((2 * width, lanes), bf16),
            vmem((tokens, lanes), f32),
            vmem((tokens, lanes), f32),
            vmem((8, lanes), f32),
            vmem((8, lanes), f32),
            vmem((8, lanes), f32),
            vmem((16 + width, lanes), f32),
            vmem((experts, rows), f32),
            vmem((experts, rows), f32),
            vmem((total, rows), bf16),
            vmem((total, rows), f32),
            vmem((rows, total), bf16),
            vmem((rows, total), bf16),
            vmem((total, half), bf16),
            vmem((Y, X, total, half), bf16),
            vmem((4 * hidden, T * half), bf16),
            vmem((Y, X, total // 4, 2 * hidden), bf16),
            vmem((total, half), bf16),
            vmem((total, half), bf16),
            vmem((Y, X, tokens, columns), bf16),
            dma((len(operands),)),
            dma((len(outs),)),
        ]
        + [dma((1,)), dma((experts, 2)), dma((1,)), dma((2,)), dma((1,)), dma((1,))]
        + [dma((5,)), dma((10, 20)), dma((2,))],
        compiler_params=pltpu.CompilerParams(
            collective_id=0, has_side_effects=True, vmem_limit_bytes=60 * 1024 * 1024
        ),
    )(*operands)
    return pl.pallas_call(
        hand_over_kernel,
        out_shape=outs,
        in_specs=[anywhere] * 2,
        out_specs=(anywhere, anywhere),
        scratch_shapes=[vmem(item.shape, item.dtype) for item in outs] + [dma((4,))],
    )(*results)


def solution(mesh, grid=None):
    n_ep, n_tp = mesh.shape["ep"], mesh.shape["tp"]
    sizes = grid or (n_ep // CORES, 4, n_tp // 4)
    Z, Y, X = sizes
    torus = Mesh(mesh.devices.reshape(Z, CORES, Y, X), AXES)
    ep, tp = ("z", "c"), ("y", "x")
    placed = (
        P(ep, tp),
        P(ep, tp),
        P(ep, tp),
        P(),
        P(),
        P(None, tp),
        P(ep, None),
        P(),
        P(ep, None),
        P(ep, None),
        P(ep, None, tp),
        P(ep, None, tp),
        P(ep, None, tp),
    )
    return jax.shard_map(
        functools.partial(on_device, sizes),
        mesh=torus,
        in_specs=placed,
        out_specs=(P(ep, tp), P(ep, tp)),
        check_vma=False,
    )
```
